32 devices in a mesh: sp: 4 (over y, x), tp: 8 (over z, core).
Axes of the slice: x: 2, y: 2, z: 4, core: 2. Of those that a mesh axis runs over, the one named last changes fastest.
Arguments:
- queries: bfloat16 [2048, 1536], P('sp', 'tp'), may hold values from -34 to 34
- latent: bfloat16 [2048, 512], P('sp'), may hold values from -6 to 6
- rot_key: bfloat16 [2048, 32], P('sp'), may hold values from -34 to 34
- latent_gain: float32 [512], replicated, may hold values from 0.1 to 1.9
- key_up: bfloat16 [512, 1024], P(None, 'tp'), may hold values from -0.25 to 0.25
- value_up: bfloat16 [512, 1024], P(None, 'tp'), may hold values from -0.70710678 to 0.70710678
- query_gain: float32 [96], replicated, may hold values from 0.5 to 6
- key_gain: float32 [96], replicated, may hold values from 0.5 to 6
- out_gain: float32 [1024], replicated, may hold values from 0.1 to 1.9
- out_weight: bfloat16 [1024, 2048], replicated, may hold values from -0.1875 to 0.1875
- residual: bfloat16 [2048, 2048], P(('sp', 'tp')), may hold values from -6 to 6
- ffn_gain: float32 [2048], replicated, may hold values from 0.1 to 1.9
- routes: int32 [2048, 2], P(('sp', 'tp')), may hold values from 0 to 3, all different within a row; in each aligned block of 64 rows (0 to 63, 64 to 127, ...) at most 36 rows name the same one
- route_weights: float32 [2048, 2], P(('sp', 'tp')), may hold values from 0.2 to 1
- expert_gate: bfloat16 [4, 2048, 2048], P('sp', None, 'tp'), may hold values from -0.125 to 0.125
- expert_up: bfloat16 [4, 2048, 2048], P('sp', None, 'tp'), may hold values from -0.125 to 0.125
- expert_down: bfloat16 [4, 2048, 2048], P('sp', 'tp'), may hold values from -0.125 to 0.125
Outputs:
- layer_out: bfloat16 [2048, 2048], P(('sp', 'tp'))
The draws below stay inside these ranges and needn't reach their ends.
Inputs may be any that keep to these rules, and one draw needn't show every extreme that they name: `routes`: the 2 experts of a token differ. Among the 64 rows of one device each expert is named by at most 36 rows, a bound that some block reaches.
All inputs are finite; a program needn't handle non-finite values.
Results may differ from the reference program's by a relative error of at most 0.02.
The reference program's roundings to bfloat16 on the way count: a program that leaves them out, or rounds other values in their place, can miss the bound.
Values may be sent and summed in bfloat16 or wider, within the bound.
No kernel may reach another device: no remote copies, remote signals or barrier semaphores. Data moves between devices by JAX's collectives and lax.ppermute only.
A program may use at most 128 MiB of HBM per device.

```python
import math
import jax
import jax.numpy as jnp
import numpy as np
from jax import lax

D = 2048
HEADS = 16
NOPE = 64
ROPE = 32
VH = 64
LAT = 512
FF_E = 2048
TOPK = 2
TOK_DEV = 64
QK = 96
ATT_WIDTH = 1024
POS_SP = 512
LENGTH = 2048
EXPERTS = 4
CAP = 36
N_SP = 4
N_TP = 8


def drawn_pair(key):
    base_query = jnp.clip(jax.random.normal(jax.random.fold_in(key, 11), (LENGTH, HEADS, QK), jnp.float32), -6.0, 6.0)
    base_key = jnp.clip(jax.random.normal(jax.random.fold_in(key, 12), (LENGTH, ROPE), jnp.float32), -6.0, 6.0)
    return (base_query.reshape(LENGTH, HEADS * QK), base_key)


def draw_queries(key, part):
    return drawn_pair(key)[0].astype(jnp.bfloat16)


def draw_rot_key(key, part):
    return drawn_pair(key)[1].astype(jnp.bfloat16)


def head_gains(key):
    spread = 1.0 + 0.18 * jax.random.uniform(jax.random.fold_in(key, 1), (QK,), jnp.float32, -2.5, 2.5)
    return spread


def draw_query_gain(key, part):
    return head_gains(jax.random.fold_in(key, 21))


def draw_key_gain(key, part):
    return head_gains(jax.random.fold_in(key, 22))


def draw_value_up(key, part):
    head_ids = jnp.arange(HEADS * VH, dtype=jnp.int32) // VH
    rising = head_ids.astype(jnp.float32) / max(HEADS - 1, 1)
    entries = jnp.clip(jax.random.normal(jax.random.fold_in(key, 32), (LAT, HEADS * VH), jnp.float32), -4.0, 4.0)
    column_scale = 3.0 ** rising
    return (entries * column_scale[None, :] / jnp.sqrt(jnp.float32(LAT))).astype(jnp.bfloat16)


def shard_levels(rng, extent, shards, smallest, top_value):
    loudness = 1.0
    for position, parts in shards:
        steps = jax.random.uniform(jax.random.fold_in(jax.random.fold_in(rng, 6), position), (parts,), jnp.float32, smallest / len(shards), top_value / len(shards))
        loudness = loudness * jnp.repeat(jnp.exp(steps), extent[position] // parts).reshape((-1,) + (1,) * (len(extent) - 1 - position))
    return loudness


def shared_out(own_key, own, number, rows, number_of, top, reach, lean):
    ranking = jax.random.permutation(own_key, number_of)
    packed, ordinary = load_shares(number_of, rows * top, reach, lean, True), load_shares(number_of, rows * top, reach, lean, False)
    places = jnp.arange(number_of)

    def named(lengths, offset_by):
        used = int((lengths > 0).sum())
        fixed = max(1, used // 4)
        moved = fixed + (places - fixed + offset_by * (used - fixed)) % max(1, number_of - fixed)
        return jnp.zeros((number_of,), jnp.int32).at[ranking[jnp.where(places < fixed, places, moved)]].set(jnp.asarray(lengths, jnp.int32))

    lengths = jnp.where(number % 4 == 0, named(packed, number // 4), named(ordinary, number - number // 4 - 1))
    mixed = jax.random.permutation(jax.random.fold_in(own, 3), number_of)
    giver, sink = mixed[0:number_of // 2 * 2:2], mixed[1:number_of // 2 * 2:2]
    slack = jnp.minimum(lengths[giver] - 1, reach - lengths[sink]) // 2
    slack = jnp.where((giver == ranking[0]) | (sink == ranking[0]) | (lengths[sink] == 0), 0, jnp.maximum(slack, 0))
    moved = jax.random.randint(jax.random.fold_in(own, 4), (number_of // 2,), 0, 1 << 20) % (slack + 1)
    lengths = lengths.at[giver].add(-moved).at[sink].add(moved)
    members = jnp.searchsorted(jnp.cumsum(lengths), jnp.arange(rows * top), side="right").astype(jnp.int32)
    listing = members.reshape(top, rows).T
    listing = listing[jax.random.permutation(jax.random.fold_in(own, 1), rows)]
    offset_by = jax.random.randint(jax.random.fold_in(own, 2), (rows, 1), 0, top)
    return jnp.take_along_axis(listing, (jnp.arange(top)[None, :] + offset_by) % top, axis=1)


def load_shares(number_of, total, bound, slope, full):
    portions = [(1 << 20) // math.isqrt(rank ** slope) + 1 for rank in range(1, number_of + 1)]
    largest = bound if full else min(bound, max(-(-total // number_of), total * portions[0] // sum(portions)))
    least = 1 if total - largest >= number_of - 1 else 0
    given, rest = [largest] + [least] * (number_of - 1), total - largest - least * (number_of - 1)
    while rest > 0:
        candidates = [i for i in range(1, number_of) if given[i] < largest] or [i for i in range(1, number_of) if given[i] < bound]
        pool, budget = sum([portions[i] for i in candidates]), rest
        for i in candidates:
            more = min(bound - given[i], max(1, budget * portions[i] // pool), rest)
            given[i] = given[i] + more
            rest = rest - more
    return np.array(given)


def bell_draw(rng, dims, deviation, bound, split=(), kind=jnp.bfloat16):
    values = deviation * jax.random.normal(rng, dims, jnp.float32)
    if split:
        values = values * shard_levels(rng, dims, split, -0.22, 0.18)
    return jnp.clip(values, -bound, bound).astype(kind)


def setup_inputs(seed: int = 0) -> dict:
    streams_of = jax.random.split(jax.random.key(seed), 18)
    queries = draw_queries(jax.random.fold_in(streams_of[17], 71), 0)
    latent = bell_draw(streams_of[1], (LENGTH, LAT), 1.0, 6.0, ((0, 4),))
    rot_key = draw_rot_key(jax.random.fold_in(streams_of[17], 71), 0)
    latent_gain = jnp.clip(1.0 + 0.18 * jax.random.normal(streams_of[3], (LAT,), jnp.float32), 0.1, 1.9)
    key_up = bell_draw(streams_of[4], (LAT, HEADS * NOPE), LAT ** -0.5, 0.25, ((1, 8),))
    value_up = draw_value_up(jax.random.fold_in(streams_of[17], 71), 0)
    query_gain = draw_query_gain(jax.random.fold_in(streams_of[17], 71), 0)
    key_gain = draw_key_gain(jax.random.fold_in(streams_of[17], 71), 0)
    out_gain = jnp.clip(1.0 + 0.18 * jax.random.normal(streams_of[8], (ATT_WIDTH,), jnp.float32), 0.1, 1.9)
    out_weight = bell_draw(streams_of[9], (ATT_WIDTH, D), ATT_WIDTH ** -0.5, 0.1875)
    residual = bell_draw(streams_of[10], (LENGTH, D), 1.0, 6.0, ((0, 32),))
    ffn_gain = jnp.clip(1.0 + 0.18 * jax.random.normal(streams_of[11], (D,), jnp.float32), 0.1, 1.9)
    routes_keys = jax.random.split(jax.random.fold_in(streams_of[12], 1), LENGTH // TOK_DEV)
    routes_turns = jax.random.permutation(jax.random.fold_in(streams_of[12], 3), LENGTH // TOK_DEV)
    routes = jax.vmap(lambda own, number: shared_out(jax.random.fold_in(streams_of[12], 2), own, number, TOK_DEV, EXPERTS, TOPK, CAP, 1))(routes_keys, routes_turns).reshape((LENGTH, TOPK))
    route_weights = jnp.clip(0.2 + 0.8 * jax.random.uniform(streams_of[13], (LENGTH, TOPK), jnp.float32) ** shard_levels(streams_of[13], (LENGTH, TOPK), ((0, 32),), -0.2, 0.2), 0.2, 1.0)
    expert_gate = bell_draw(streams_of[14], (EXPERTS, D, FF_E), D ** -0.5, 0.125, ((0, 4), (2, 8)))
    expert_up = bell_draw(streams_of[15], (EXPERTS, D, FF_E), D ** -0.5, 0.125, ((0, 4), (2, 8)))
    expert_down = bell_draw(streams_of[16], (EXPERTS, FF_E, D), FF_E ** -0.5, 0.125, ((0, 4), (1, 8)))
    return dict(queries=queries, latent=latent, rot_key=rot_key, latent_gain=latent_gain, key_up=key_up, value_up=value_up, query_gain=query_gain, key_gain=key_gain, out_gain=out_gain, out_weight=out_weight, residual=residual, ffn_gain=ffn_gain, routes=routes, route_weights=route_weights, expert_gate=expert_gate, expert_up=expert_up, expert_down=expert_down)


epsilon = 1e-06
rope_base = 10000.0

def rms_scale(values):
    return lax.rsqrt(lax.optimization_barrier(jnp.mean(values * values, axis=-1, keepdims=True)) + epsilon)

def rotate_half(values, angles):
    half_dims = values.shape[-1] // 2
    first_half = values[..., :half_dims]
    second_half = values[..., half_dims:]
    cosine = jnp.cos(angles)
    sine_val = jnp.sin(angles)
    return jnp.concatenate([first_half * cosine - second_half * sine_val, second_half * cosine + first_half * sine_val], axis=-1)

def head_prepare(raw_rows, gain_vec, angles):
    normed_rows = raw_rows * rms_scale(raw_rows) * gain_vec
    turned_rows = rotate_half(normed_rows[..., NOPE:], angles[:, None, :])
    return jnp.concatenate([normed_rows[..., :NOPE], turned_rows], axis=-1).astype(jnp.bfloat16)

def attend_head(head_inputs):
    query_head, key_head, value_head = head_inputs
    query_f32 = query_head.astype(jnp.float32)
    key_f32 = key_head.astype(jnp.float32)
    value_f32 = value_head.astype(jnp.float32)
    block_count = LENGTH // POS_SP
    query_blocks = query_f32.reshape(block_count, POS_SP, QK)
    key_pos = jnp.arange(LENGTH, dtype=jnp.int32)

    def one_block(block_inputs):
        block_index, query_block = block_inputs
        scores = jnp.dot(query_block, key_f32.T, precision=lax.Precision.HIGHEST) * QK ** (-0.5)
        query_pos = block_index * POS_SP + jnp.arange(POS_SP, dtype=jnp.int32)
        allowed = key_pos[None, :] <= query_pos[:, None]
        scores = jnp.where(allowed, scores, -1e+30)
        row_peak = lax.optimization_barrier(jnp.max(scores, axis=1, keepdims=True))
        exponent = jnp.where(allowed, jnp.exp(scores - row_peak), 0.0)
        row_total = lax.optimization_barrier(jnp.sum(exponent, axis=1))
        rounded_exp = lax.optimization_barrier(exponent.astype(jnp.bfloat16)).astype(jnp.float32)
        result = jnp.dot(rounded_exp, value_f32, precision=lax.Precision.HIGHEST) / row_total[:, None]
        return result.astype(jnp.bfloat16)
    outputs = lax.map(one_block, (jnp.arange(block_count, dtype=jnp.int32), query_blocks))
    return outputs.reshape(LENGTH, VH)

def reference(queries, latent, rot_key, latent_gain, key_up, value_up, query_gain, key_gain, out_gain, out_weight, residual, ffn_gain, routes, route_weights, expert_gate, expert_up, expert_down):
    lat_f32 = latent.astype(jnp.float32)
    normed_latent = (lat_f32 * rms_scale(lat_f32) * latent_gain).astype(jnp.bfloat16)
    key_nope = jnp.dot(normed_latent, key_up, preferred_element_type=jnp.float32).astype(jnp.bfloat16)
    values = jnp.dot(normed_latent, value_up, preferred_element_type=jnp.float32).astype(jnp.bfloat16)
    positions = jnp.arange(LENGTH, dtype=jnp.int32)
    inverse = rope_base ** (-jnp.arange(0, ROPE, 2, dtype=jnp.float32) / ROPE)
    angles = positions.astype(jnp.float32)[:, None] * inverse[None, :]
    shared = jnp.broadcast_to(rot_key.astype(jnp.float32)[:, None, :], (LENGTH, HEADS, ROPE))
    raw_keys = jnp.concatenate([key_nope.astype(jnp.float32).reshape(LENGTH, HEADS, NOPE), shared], axis=-1)
    key_rows = head_prepare(raw_keys, key_gain, angles)
    query_rows = head_prepare(queries.astype(jnp.float32).reshape(LENGTH, HEADS, QK), query_gain, angles)
    value_heads = values.reshape(LENGTH, HEADS, VH)
    attended = lax.map(attend_head, (jnp.transpose(query_rows, (1, 0, 2)), jnp.transpose(key_rows, (1, 0, 2)), jnp.transpose(value_heads, (1, 0, 2))))
    att_rows = jnp.transpose(attended, (1, 0, 2)).reshape(LENGTH, ATT_WIDTH).astype(jnp.float32)
    normed_att = (att_rows * rms_scale(att_rows) * out_gain).astype(jnp.bfloat16)
    group_width = ATT_WIDTH // N_TP
    mixed = jnp.zeros((LENGTH, D), jnp.float32)
    for group_index in range(N_TP):
        low = group_index * group_width
        partial_value = jnp.dot(normed_att[:, low:low + group_width], out_weight[low:low + group_width], preferred_element_type=jnp.float32).astype(jnp.bfloat16)
        mixed = mixed + lax.optimization_barrier(partial_value).astype(jnp.float32)
    middle = residual.astype(jnp.float32) + mixed
    ffn_input = (middle * rms_scale(middle) * ffn_gain).astype(jnp.bfloat16)
    flat_routes = routes.reshape(-1).astype(jnp.int32)
    row_order = jnp.argsort(flat_routes, stable=True).astype(jnp.int32)
    expert_counts = lax.optimization_barrier(jnp.sum((flat_routes[:, None] == jnp.arange(EXPERTS, dtype=jnp.int32)[None, :]).astype(jnp.int32), axis=0))
    offsets = (jnp.cumsum(expert_counts) - expert_counts).astype(jnp.int32)
    row_limit = N_SP * N_TP * CAP
    weights_flat = route_weights.reshape(-1).astype(jnp.float32)
    hidden_width = FF_E // N_TP

    def per_expert(expert_id, combined):
        slot_ids = jnp.arange(row_limit, dtype=jnp.int32)
        is_live = slot_ids < expert_counts[expert_id]
        picked = row_order[jnp.minimum(offsets[expert_id] + slot_ids, LENGTH * TOPK - 1)]
        token_ids = (picked // TOPK).astype(jnp.int32)
        expert_in = ffn_input[token_ids]
        gate_pre = jnp.dot(expert_in, expert_gate[expert_id], preferred_element_type=jnp.float32)
        up_pre = jnp.dot(expert_in, expert_up[expert_id], preferred_element_type=jnp.float32)
        hidden = (jax.nn.silu(gate_pre) * up_pre).astype(jnp.bfloat16)
        down_weight = expert_down[expert_id]
        down_sum = jnp.zeros((row_limit, D), jnp.float32)
        for group_index in range(N_TP):
            low = group_index * hidden_width
            partial_value = jnp.dot(hidden[:, low:low + hidden_width], down_weight[low:low + hidden_width], preferred_element_type=jnp.float32).astype(jnp.bfloat16)
            down_sum = down_sum + lax.optimization_barrier(partial_value).astype(jnp.float32)
        expert_out = lax.optimization_barrier(down_sum.astype(jnp.bfloat16)).astype(jnp.float32)
        contrib_rows = expert_out * (weights_flat[picked] * is_live.astype(jnp.float32))[:, None]
        return combined.at[token_ids].add(contrib_rows)
    combined = lax.fori_loop(0, EXPERTS, per_expert, jnp.zeros((LENGTH, D), jnp.float32))
    return (middle + combined).astype(jnp.bfloat16)
```

```python
import functools

import jax
import jax.numpy as jnp
import numpy as np
from jax import lax
from jax.experimental import pallas as pl
from jax.experimental.pallas import tpu as pltpu
from jax.sharding import PartitionSpec as P

NOPE = 64
ROPE = 32
VH = 64
TOPK = 2
QK = 96
LANES = 128
COL_CHUNKS = 2


epsilon = 1e-06
rope_base = 10000.0
f32 = jnp.float32
bf16 = jnp.bfloat16


def dot(a, b):
    return jnp.dot(a, b, preferred_element_type=f32)


def rope_select(offset, rows):
    direct = np.zeros((rows, LANES), np.float32)
    turned = np.zeros((rows, LANES), np.float32)
    half = ROPE // 2
    for lane in range(LANES):
        d = lane % ROPE
        direct[offset + d, lane] = 1.0
        turned[offset + (d + half) % ROPE, lane] = -1.0 if d < half else 1.0
    return direct, turned


def query_select(heads):
    parts = []
    for h in range(heads):
        nope = np.zeros((heads * QK, LANES), np.float32)
        for i in range(NOPE):
            nope[h * QK + i, i] = 1.0
        parts += [nope, *rope_select(h * QK + NOPE, heads * QK)]
    return np.concatenate(parts, axis=1)


def gain_rows(gain):
    rope_gain = gain[NOPE:]
    nope = jnp.concatenate([gain[:NOPE], jnp.zeros((LANES - NOPE,), f32)])
    direct = jnp.tile(rope_gain, LANES // ROPE)
    turned = jnp.tile(jnp.roll(rope_gain, ROPE // 2), LANES // ROPE)
    return [nope, direct, turned]


def prep_kernel(
    heads, lat, rot, lat_gain, key_up, value_up, queries, gains, cosine, sine, selq, selk,
    bundle, q1, q2,
):
    rows = lat.shape[0]
    pack = LANES // (ROPE * heads)
    sub = rows // pack
    x = lat[...].astype(f32)
    scale = lax.rsqrt(jnp.mean(x * x, axis=-1, keepdims=True) + epsilon)
    normed = (x * scale * lat_gain[...]).astype(bf16)
    cos, sin = cosine[...], sine[...]
    lane = lax.broadcasted_iota(jnp.int32, (rows, LANES), 1)
    is_key = lane < NOPE
    turns = dot(rot[...], selk[...])
    rot_a, rot_b = turns[:, :LANES], turns[:, LANES:]
    rot_sq = jnp.sum(rot_a * rot_a, axis=-1, keepdims=True) * (ROPE / LANES)
    spun = rot_a * gains[4:5, :] * cos + rot_b * gains[5:6, :] * sin
    key_scales = None
    for h in range(heads):
        weight = jnp.concatenate(
            [key_up[:, h * NOPE : (h + 1) * NOPE], value_up[:, h * VH : (h + 1) * VH]], axis=1
        )
        kv = dot(normed, weight).astype(bf16).astype(f32)
        sq = jnp.sum(jnp.where(is_key, kv * kv, 0.0), axis=-1, keepdims=True) + rot_sq
        r = lax.rsqrt(sq * (1.0 / QK) + epsilon)
        bundle[h * rows : (h + 1) * rows, :] = jnp.where(
            is_key, kv * r * gains[3:4, :], kv
        ).astype(bf16)
        spread = jnp.broadcast_to(r, (rows, LANES))
        key_scales = (
            spread
            if key_scales is None
            else jnp.where((lane // ROPE) % heads == h, spread, key_scales)
        )
    spun = spun * key_scales
    tile = spun[:sub]
    for p in range(1, pack):
        tile = jnp.where(
            lane[:sub] // (ROPE * heads) == p, spun[p * sub : (p + 1) * sub], tile
        )
    bundle[heads * rows :, :] = tile.astype(bf16)
    picked = dot(queries[...], selq[...])
    for h in range(heads):
        base = h * 3 * LANES
        nope = picked[:, base : base + LANES]
        qa = picked[:, base + LANES : base + 2 * LANES]
        qb = picked[:, base + 2 * LANES : base + 3 * LANES]
        sq = jnp.sum(nope * nope + qa * qa * (ROPE / LANES), axis=-1, keepdims=True)
        r = lax.rsqrt(sq * (1.0 / QK) + epsilon)
        q1[h] = (nope * r * gains[0:1, :]).astype(bf16)
        turned = (qa * gains[1:2, :] * cos + qb * gains[2:3, :] * sin) * r
        for p in range(pack):
            q2[h * pack + p] = jnp.where(lane // ROPE == p * heads + h, turned, 0.0).astype(bf16)


def attend_kernel(heads, tokens, groups, scal, q1, q2, *refs):
    sources = len(refs) - 6
    bundles = refs[:sources]
    keep, send, peak_ref, total_ref, acc_ref, result = refs[sources:]
    rows = q1.shape[1]
    pack = LANES // (ROPE * heads)
    sub = rows // pack
    factor = float(QK ** (-0.5) * np.log2(np.e))
    me, core = scal[0], scal[2]

    def block(h, source, masked):
        ref = bundles[source]
        parts = []
        for p in range(pack):
            query = jnp.concatenate([q1[h], q2[h * pack + p]], axis=1)
            key = jnp.concatenate(
                [
                    ref[h * rows + p * sub : h * rows + (p + 1) * sub, :],
                    ref[heads * rows : heads * rows + sub, :],
                ],
                axis=1,
            )
            parts.append(
                lax.dot_general(query, key, (((1,), (1,)), ((), ())), preferred_element_type=f32)
            )
        scores = jnp.concatenate(parts, axis=1)
        if masked:
            row = lax.broadcasted_iota(jnp.int32, (rows, rows), 0)
            col = lax.broadcasted_iota(jnp.int32, (rows, rows), 1)
            scores = jnp.where(col <= row, scores, -1e30)
        top = jnp.max(scores, axis=1, keepdims=True)
        if masked:
            peak = top
        else:
            before = peak_ref[h]
            peak = jnp.maximum(before, top)
            fade = jnp.exp2((before - peak) * factor)
        weights = jnp.exp2((scores - peak) * factor)
        total = jnp.sum(weights, axis=1, keepdims=True)
        part = dot(weights.astype(bf16), ref[h * rows : (h + 1) * rows, :])
        if not masked:
            total = total + total_ref[h] * fade
            part = part + acc_ref[h] * fade
        peak_ref[h] = peak
        total_ref[h] = total
        acc_ref[h] = part

    for h in range(heads):
        block(h, 0, True)
    for source in range(1, sources):

        @pl.when((me ^ source) < me)
        def _():
            for h in range(heads):
                block(h, source, False)

    outs = [acc_ref[h][:, NOPE:] / total_ref[h] for h in range(heads)]
    result[...] = outs[0] if heads == 1 else jnp.concatenate(outs, axis=1)
    for g in range(groups):
        at = g * 2 * tokens
        keep[g * tokens : (g + 1) * tokens, :] = result[
            pl.ds(pl.multiple_of(at + core * tokens, tokens), tokens), :
        ].astype(bf16)
        send[g * tokens : (g + 1) * tokens, :] = result[
            pl.ds(pl.multiple_of(at + (1 - core) * tokens, tokens), tokens), :
        ].astype(bf16)


def choose_kernel(groups, tokens, scal, gain, chooser, *refs):
    pieces = refs[: 2 * groups]
    outs = refs[2 * groups : -3]
    own, rows_ref, normed_ref = refs[-3:]
    z, core = scal[1], scal[2]
    width = 2 * pieces[0].shape[1]
    for g in range(groups):
        mine, other = pieces[2 * g][...].astype(f32), pieces[2 * g + 1][...].astype(f32)
        first = jnp.where(core == 0, mine, other)
        second = jnp.where(core == 0, other, mine)
        at = pl.multiple_of((z ^ g) * width, width)
        rows_ref[:, pl.ds(at, width)] = jnp.concatenate([first, second], axis=1)
    x = rows_ref[...]
    scale = lax.rsqrt(jnp.mean(x * x, axis=-1, keepdims=True) + epsilon)
    normed_ref[...] = (x * scale * gain[...]).astype(bf16)
    slots = outs[0].shape[0]
    for k, out in enumerate(outs):
        out[...] = dot(chooser[k * slots : (k + 1) * slots, :], normed_ref[...]).astype(bf16)
    own[...] = normed_ref[pl.ds(pl.multiple_of(z * tokens, tokens), tokens), :]


def expert_kernel(
    count, out_weight, ffn_gain, gate_a, up_a, down_a, gate_b, up_b, down_b, *refs
):
    resids, norms, row_weights = refs[:count], refs[count : 2 * count], refs[2 * count : 3 * count]
    outs = refs[3 * count :]
    chunks = len(outs) // count
    slots = resids[0].shape[0]
    join = lambda parts: parts[0][...] if count == 1 else jnp.concatenate([p[...] for p in parts])
    middle = join(resids).astype(f32) + dot(join(norms), out_weight[...])
    scale = lax.rsqrt(jnp.mean(middle * middle, axis=-1, keepdims=True) + epsilon)
    x = (middle * scale * ffn_gain[...]).astype(bf16)
    hiddens = []
    for gate, up in ((gate_a, up_a), (gate_b, up_b)):
        g = dot(x, gate[0])
        u = dot(x, up[0])
        hiddens.append((g / (1.0 + jnp.exp(-g)) * u).astype(bf16))
    weight = join(row_weights)[:, :1]
    width = outs[0].shape[1]
    for j in range(chunks):
        cols = slice(j * width, (j + 1) * width)
        out = dot(hiddens[0], down_a[0, :, cols]) + dot(hiddens[1], down_b[0, :, cols])
        out = (out * weight).astype(bf16)
        for i in range(count):
            outs[i * chunks + j][...] = out[i * slots : (i + 1) * slots]


def combine_kernel(sources, tokens, gather, *refs):
    rows, outs = refs[:sources], refs[sources:]
    slots = rows[0].shape[0]
    total = None
    for k in range(sources):
        part = dot(gather[:, k * slots : (k + 1) * slots], rows[k][...])
        total = part if total is None else total + part
    for g, out in enumerate(outs):
        out[...] = total[g * tokens : (g + 1) * tokens].astype(out.dtype)


VM = pl.BlockSpec(memory_space=pltpu.VMEM)
SM = pl.BlockSpec(memory_space=pltpu.SMEM)


def call(body, args, outs, scratch=(), scalars=0, flops=0, trans=0):
    size = lambda a: int(np.prod(a.shape)) * a.dtype.itemsize
    return pl.pallas_call(
        body,
        out_shape=outs,
        in_specs=[SM] * scalars + [VM] * (len(args) - scalars),
        out_specs=jax.tree.map(lambda _: VM, outs),
        scratch_shapes=list(scratch),
        cost_estimate=pl.CostEstimate(
            flops=int(flops),
            transcendentals=int(trans),
            bytes_accessed=sum(size(a) for a in args) + sum(size(o) for o in jax.tree.leaves(outs)),
        ),
        compiler_params=pltpu.CompilerParams(vmem_limit_bytes=56 * 1024 * 1024),
    )(*args)


def shape(dims, dtype):
    return jax.ShapeDtypeStruct(tuple(dims), dtype)


def slot_table(route_blocks, weight_blocks, block_ids, wanted, cap):
    groups, tokens, _ = route_blocks.shape
    hits = route_blocks[..., None] == wanted[None, None, None, :]
    hit = jnp.any(hits, axis=2)
    weight = jnp.sum(jnp.where(hits, weight_blocks[..., None], 0.0), axis=2)
    before = jnp.asarray(np.tril(np.ones((tokens, tokens), np.float32), -1), bf16)
    rank = jnp.einsum("ij,gje->gie", before, hit.astype(bf16), preferred_element_type=f32)
    slot = rank.astype(jnp.int32) + (block_ids * cap)[:, None, None]
    slot = jnp.where(hit, slot, -1).reshape(groups * tokens, -1)
    return slot, weight.reshape(groups * tokens, -1)


def shards(
    queries, latent, rot_key, latent_gain, key_up, value_up, query_gain, key_gain, out_gain,
    out_weight, residual, ffn_gain, routes, route_weights, expert_gate, expert_up, expert_down,
):
    rows = queries.shape[0]
    heads = key_up.shape[1] // NOPE
    width = residual.shape[1]
    sp, tp = lax.axis_size("sp"), lax.axis_size("tp")
    groups = tp // 2
    tokens = residual.shape[0]
    all_tokens = groups * tokens
    att_width = out_weight.shape[0]
    me, place = lax.axis_index("sp"), lax.axis_index("tp")
    z, core = place // 2, place % 2
    scal = jnp.stack([me, z, core]).astype(jnp.int32)
    cap = max(2, 9 * tokens * TOPK // (8 * sp))
    slots = groups * cap

    swap_core = lambda v: lax.ppermute(v, "tp", [(i, i ^ 1) for i in range(tp)])
    swap_z = lambda v, k: lax.ppermute(v, "tp", [(i, i ^ (2 * k)) for i in range(tp)])
    swap_sp = lambda v, k: lax.ppermute(v, "sp", [(i, i ^ k) for i in range(sp)])

    positions = (me * rows + jnp.arange(rows, dtype=jnp.int32)).astype(f32)
    inverse = rope_base ** (-jnp.arange(0, ROPE, 2, dtype=f32) / ROPE)
    angles = positions[:, None] * jnp.tile(inverse, 2 * LANES // ROPE)[None, :]
    pack = LANES // (ROPE * heads)
    gains = jnp.stack(gain_rows(query_gain) + gain_rows(key_gain))
    selk = jnp.asarray(np.concatenate(rope_select(0, ROPE), axis=1), bf16)
    selq = jnp.asarray(query_select(heads), bf16)
    bundle_rows = heads * rows + rows // pack
    bundle, q1, q2 = call(
        functools.partial(prep_kernel, heads),
        [
            latent, rot_key, latent_gain[None, :], key_up, value_up, queries, gains,
            jnp.cos(angles), jnp.sin(angles), selq, selk,
        ],
        (
            shape((bundle_rows, LANES), bf16),
            shape((heads, rows, LANES), bf16),
            shape((heads * pack, rows, LANES), bf16),
        ),
        flops=2 * rows * latent.shape[1] * 256 + 2 * rows * 192 * 768,
    )
    bundles = [bundle] + [swap_sp(bundle, k) for k in range(1, sp)]

    resid_all = jnp.concatenate([residual] + [swap_z(residual, k) for k in range(1, groups)])
    tickets = jnp.concatenate([routes.astype(f32), route_weights], axis=1)
    ticket_blocks = jnp.stack([tickets] + [swap_z(tickets, k) for k in range(1, groups)])
    gate_b, up_b, down_b = swap_core(expert_gate), swap_core(expert_up), swap_core(expert_down)
    wanted = me ^ jnp.arange(sp, dtype=jnp.int32)
    block_ids = z ^ jnp.arange(groups, dtype=jnp.int32)
    route_blocks = ticket_blocks[..., :TOPK].astype(jnp.int32)
    slot_rel, weight_rel = slot_table(
        route_blocks, ticket_blocks[..., TOPK:], block_ids, wanted, cap
    )
    slot_ids = jnp.arange(slots, dtype=jnp.int32)
    choose_rel = slot_rel.T[:, None, :] == slot_ids[None, :, None]
    slot_glob = jnp.concatenate(
        [
            lax.dynamic_slice_in_dim(slot_rel, (z ^ g) * tokens, tokens, 0)
            for g in range(groups)
        ]
    )
    choose_glob = (
        (slot_glob.T[:, None, :] == slot_ids[None, :, None])
        .astype(bf16)
        .reshape(sp * slots, all_tokens)
    )
    gather_rel = (
        (slot_rel[:, :, None] == slot_ids[None, None, :])
        .astype(bf16)
        .reshape(all_tokens, sp * slots)
    )
    row_weight = jnp.sum(jnp.where(choose_rel, weight_rel.T[:, None, :], 0.0), axis=2)
    row_weight = jnp.broadcast_to(row_weight[:, :, None], (sp, slots, LANES))
    resid_rows = dot(
        choose_rel.astype(bf16).reshape(sp * slots, all_tokens), resid_all
    ).astype(bf16)
    resid_rows = [resid_rows[k * slots : (k + 1) * slots] for k in range(sp)]
    resid_in = [resid_rows[0]] + [swap_sp(resid_rows[k], k) for k in range(1, sp)]
    weight_in = [row_weight[0]] + [swap_sp(row_weight[k], k) for k in range(1, sp)]

    half = heads * VH
    keep, send = call(
        functools.partial(attend_kernel, heads, tokens, groups),
        [scal, q1, q2] + bundles,
        (shape((all_tokens, half), bf16), shape((all_tokens, half), bf16)),
        [
            pltpu.VMEM((heads, rows, 1), f32),
            pltpu.VMEM((heads, rows, 1), f32),
            pltpu.VMEM((heads, rows, LANES), f32),
            pltpu.VMEM((rows, half), f32),
        ],
        scalars=1,
        flops=2 * heads * rows * rows * sp * 384,
        trans=heads * rows * rows * sp,
    )
    other = swap_core(send)
    pieces = [keep, other]
    kept_in = [swap_z(keep, k) for k in range(1, groups)]
    other_in = [swap_z(other, k) for k in range(1, groups)]
    for a, b in zip(kept_in, other_in):
        pieces += [a, b]
    *norm_rows, own_rows = call(
        functools.partial(choose_kernel, groups, tokens),
        [scal, out_gain[None, :], choose_glob] + pieces,
        tuple([shape((slots, att_width), bf16)] * sp) + (shape((tokens, att_width), bf16),),
        [pltpu.VMEM((all_tokens, att_width), f32), pltpu.VMEM((all_tokens, att_width), bf16)],
        scalars=1,
        flops=2 * sp * slots * all_tokens * att_width,
    )
    norm_in = [norm_rows[0]] + [swap_sp(norm_rows[k], k) for k in range(1, sp)]
    middle = residual.astype(f32) + dot(own_rows, out_weight)

    hidden = 2 * expert_gate.shape[2]
    chunk = width // COL_CHUNKS
    served = [None] * sp
    for part in ([0], [1, 2], list(range(3, sp))):
        outs = call(
            functools.partial(expert_kernel, len(part)),
            [
                out_weight, ffn_gain[None, :], expert_gate, expert_up, expert_down,
                gate_b, up_b, down_b,
            ]
            + [resid_in[k] for k in part]
            + [norm_in[k] for k in part]
            + [weight_in[k] for k in part],
            tuple([shape((slots, chunk), bf16)] * (len(part) * COL_CHUNKS)),
            flops=2 * len(part) * slots * width * (att_width + 3 * hidden),
        )
        for i, k in enumerate(part):
            served[k] = outs[i * COL_CHUNKS : (i + 1) * COL_CHUNKS]
    finished = []
    for j in range(COL_CHUNKS):
        back = [served[0][j]] + [swap_sp(served[k][j], k) for k in range(1, sp)]
        own, *rest = call(
            functools.partial(combine_kernel, sp, tokens),
            [gather_rel] + back,
            (shape((tokens, chunk), f32),) + tuple([shape((tokens, chunk), bf16)] * (groups - 1)),
            flops=2 * all_tokens * sp * slots * chunk,
        )
        total = middle[:, j * chunk : (j + 1) * chunk] + own
        for k in range(1, groups):
            total = total + swap_z(rest[k - 1], k).astype(f32)
        finished.append(total.astype(bf16))
    return jnp.concatenate(finished, axis=1)


def solution(mesh):
    return jax.shard_map(
        shards,
        mesh=mesh,
        in_specs=(
            P("sp", "tp"),
            P("sp", None),
            P("sp", None),
            P(),
            P(None, "tp"),
            P(None, "tp"),
            P(),
            P(),
            P(),
            P(),
            P(("sp", "tp"), None),
            P(),
            P(("sp", "tp"), None),
            P(("sp", "tp"), None),
            P("sp", None, "tp"),
            P("sp", None, "tp"),
            P("sp", "tp", None),
        ),
        out_specs=P(("sp", "tp"), None),
        check_vma=False,
    )
```

```python
import functools

import jax
import jax.numpy as jnp
import numpy as np
from jax import lax
from jax.experimental import pallas as pl
from jax.experimental.pallas import tpu as pltpu
from jax.sharding import PartitionSpec as P


NOPE = 64
ROPE = 32
VH = 64
TOPK = 2
QK = 96
LANES = 128
COL_CHUNKS = 2
ROOM = 60


epsilon = 1e-06
rope_base = 10000.0
f32 = jnp.float32
bf16 = jnp.bfloat16


def dot(a, b):
    return jnp.dot(a, b, preferred_element_type=f32)


def rope_select(offset, rows):
    direct = np.zeros((rows, LANES), np.float32)
    turned = np.zeros((rows, LANES), np.float32)
    half = ROPE // 2
    for lane in range(LANES):
        d = lane % ROPE
        direct[offset + d, lane] = 1.0
        turned[offset + (d + half) % ROPE, lane] = -1.0 if d < half else 1.0
    return direct, turned


def head_select(heads):
    parts = []
    for h in range(heads):
        nope = np.zeros((heads * QK, LANES), np.float32)
        for i in range(NOPE):
            nope[h * QK + i, i] = 1.0
        parts += [nope, *rope_select(h * QK + NOPE, heads * QK)]
    return np.concatenate(parts, axis=1)


def turn_tables(rows, blocks):
    inverse = rope_base ** (-np.arange(0, ROPE, 2, dtype=np.float64) / ROPE)
    inverse = np.tile(inverse, 2 * LANES // ROPE)[None, :]
    inner = np.arange(rows, dtype=np.float64)[:, None] * inverse
    first = np.arange(blocks, dtype=np.float64)[:, None] * rows * inverse
    return [
        np.concatenate([np.cos(a), np.sin(a)], axis=1).astype(np.float32) for a in (inner, first)
    ]


def dot_rows(a, b):
    return lax.dot_general(a, b, (((0,), (0,)), ((), ())), preferred_element_type=f32)


def prep_kernel(
    heads, lat, rot, lat_gain, key_up, value_up, queries, q_gain, k_gain, inner, first,
    selq, selk, selg, bundle, q1, q2,
):
    rows = lat.shape[0]
    pack = LANES // (ROPE * heads)
    sub = rows // pack
    me = lax.axis_index("sp")
    x = lat[...].astype(f32)
    scale = lax.rsqrt(jnp.mean(x * x, axis=-1, keepdims=True) + epsilon)
    normed = (x * scale * lat_gain[...]).astype(bf16)
    base = first[pl.ds(me, 1), :]
    base_cos, base_sin = base[:, :LANES], base[:, LANES:]
    in_cos, in_sin = inner[:, :LANES], inner[:, LANES:]
    cos = in_cos * base_cos - in_sin * base_sin
    sin = in_sin * base_cos + in_cos * base_sin
    spread_gain = lambda g: jnp.dot(
        g[...], selg[...], precision=lax.Precision.HIGHEST, preferred_element_type=f32
    )
    gq, gk = spread_gain(q_gain), spread_gain(k_gain)
    cut = lambda g, i: g[:, i * LANES : (i + 1) * LANES]
    lane = lax.broadcasted_iota(jnp.int32, (rows, LANES), 1)
    is_key = lane < NOPE
    turns = dot_rows(rot[...], selk[...])
    rot_a, rot_b = turns[:, :LANES], turns[:, LANES:]
    rot_sq = jnp.sum(rot_a * rot_a, axis=-1, keepdims=True) * (ROPE / LANES)
    spun = rot_a * cut(gk, 1) * cos + rot_b * cut(gk, 2) * sin
    key_scales = None
    for h in range(heads):
        weight = jnp.concatenate(
            [key_up[:, h * NOPE : (h + 1) * NOPE], value_up[:, h * VH : (h + 1) * VH]], axis=1
        )
        kv = dot(normed, weight).astype(bf16).astype(f32)
        sq = jnp.sum(jnp.where(is_key, kv * kv, 0.0), axis=-1, keepdims=True) + rot_sq
        r = lax.rsqrt(sq * (1.0 / QK) + epsilon)
        bundle[h * rows : (h + 1) * rows, :] = jnp.where(
            is_key, kv * r * cut(gk, 0), kv
        ).astype(bf16)
        spread = jnp.broadcast_to(r, (rows, LANES))
        key_scales = (
            spread
            if key_scales is None
            else jnp.where((lane // ROPE) % heads == h, spread, key_scales)
        )
    spun = spun * key_scales
    tile = spun[:sub]
    for p in range(1, pack):
        tile = jnp.where(
            lane[:sub] // (ROPE * heads) == p, spun[p * sub : (p + 1) * sub], tile
        )
    bundle[heads * rows :, :] = tile.astype(bf16)
    picked = dot_rows(queries[...], selq[...])
    for h in range(heads):
        base = h * 3 * LANES
        nope = picked[:, base : base + LANES]
        qa = picked[:, base + LANES : base + 2 * LANES]
        qb = picked[:, base + 2 * LANES : base + 3 * LANES]
        sq = jnp.sum(nope * nope + qa * qa * (ROPE / LANES), axis=-1, keepdims=True)
        r = lax.rsqrt(sq * (1.0 / QK) + epsilon)
        q1[h] = (nope * r * cut(gq, 0)).astype(bf16)
        turned = (qa * cut(gq, 1) * cos + qb * cut(gq, 2) * sin) * r
        for p in range(pack):
            q2[h * pack + p] = jnp.where(lane // ROPE == p * heads + h, turned, 0.0).astype(bf16)


def scores_of(heads, q1, q2, ref, h, top, count, parts):
    rows = q1.shape[1]
    pack = LANES // (ROPE * heads)
    sub = rows // pack
    out = []
    for p in range(parts):
        query = jnp.concatenate(
            [q1[h, top : top + count], q2[h * pack + p, top : top + count]], axis=1
        )
        key = jnp.concatenate(
            [
                ref[h * rows + p * sub : h * rows + (p + 1) * sub, :],
                ref[heads * rows : heads * rows + sub, :],
            ],
            axis=1,
        )
        out.append(
            lax.dot_general(key, query, (((1,), (1,)), ((), ())), preferred_element_type=f32)
        )
    return out[0] if parts == 1 else jnp.concatenate(out, axis=0)


FACTOR = float(QK ** (-0.5) * np.log2(np.e))


def attend_own(heads, q1, q2, ref, state):
    rows = q1.shape[1]
    pack = LANES // (ROPE * heads)
    sub = rows // pack
    for h in range(heads):
        for b in range(pack):
            scores = scores_of(heads, q1, q2, ref, h, b * sub, sub, b + 1)
            key = lax.broadcasted_iota(jnp.int32, scores.shape, 0)
            query = lax.broadcasted_iota(jnp.int32, scores.shape, 1) + b * sub
            scores = jnp.where(key <= query, scores, -1e30)
            peak = jnp.max(scores, axis=0, keepdims=True)
            weights = jnp.exp2((scores - peak) * FACTOR)
            total = jnp.sum(weights, axis=0, keepdims=True)
            part = dot_rows(ref[h * rows : h * rows + (b + 1) * sub, :], weights.astype(bf16))
            row = lax.broadcasted_iota(jnp.int32, part.shape, 0)
            state[h, :, b * sub : (b + 1) * sub] = jnp.where(
                row == 0, peak, jnp.where(row == 1, total, part)
            )


def attend_other(heads, q1, q2, ref, state):
    rows = q1.shape[1]
    pack = LANES // (ROPE * heads)
    for h in range(heads):
        scores = scores_of(heads, q1, q2, ref, h, 0, rows, pack)
        old = state[h, 0:1, :]
        peak = jnp.maximum(old, jnp.max(scores, axis=0, keepdims=True))
        fade = jnp.exp2((old - peak) * FACTOR)
        weights = jnp.exp2((scores - peak) * FACTOR)
        total = state[h, 1:2, :] * fade + jnp.sum(weights, axis=0, keepdims=True)
        part = dot_rows(ref[h * rows : (h + 1) * rows, :], weights.astype(bf16))
        part = part + state[h] * fade
        row = lax.broadcasted_iota(jnp.int32, part.shape, 0)
        state[h] = jnp.where(row == 0, peak, jnp.where(row == 1, total, part))


def attend_first_kernel(heads, sources, q1, q2, *refs):
    bundles, state = refs[: len(sources)], refs[-1]
    me = lax.axis_index("sp")
    attend_own(heads, q1, q2, bundles[0], state)
    for i, k in enumerate(sources):
        if k:

            @pl.when((me ^ k) < me)
            def _():
                attend_other(heads, q1, q2, bundles[i], state)


def attend_last_kernel(heads, tokens, groups, sources, q1, q2, before, *refs):
    bundles = refs[: len(sources)]
    keep, send, state, result = refs[len(sources) :]
    me = lax.axis_index("sp")
    core = lax.axis_index("tp") % 2
    state[...] = before[...]
    for i, k in enumerate(sources):

        @pl.when((me ^ k) < me)
        def _():
            attend_other(heads, q1, q2, bundles[i], state)

    outs = [state[h, NOPE:, :] / state[h, 1:2, :] for h in range(heads)]
    result[...] = (outs[0] if heads == 1 else jnp.concatenate(outs, axis=0)).T
    for g in range(groups):
        at = g * 2 * tokens
        keep[g * tokens : (g + 1) * tokens, :] = result[
            pl.ds(pl.multiple_of(at + core * tokens, tokens), tokens), :
        ].astype(bf16)
        send[g * tokens : (g + 1) * tokens, :] = result[
            pl.ds(pl.multiple_of(at + (1 - core) * tokens, tokens), tokens), :
        ].astype(bf16)


def pack_kernel(routes, weights, residual, flags, first, second):
    half = second.shape[1]
    rows = [routes[...].astype(f32)]
    for j in range(TOPK):
        rest = weights[j : j + 1, :]
        for _ in range(3):
            piece = rest.astype(bf16).astype(f32)
            rows.append(piece)
            rest = rest - piece
    stacked = jnp.concatenate(rows, axis=0)
    first[:, :half] = residual[:, :half]
    first[:, half:] = dot_rows(stacked.astype(bf16), flags[...]).astype(bf16)
    second[...] = residual[:, half:]


def residual_first_kernel(groups, sp, cap, lower, *refs):
    parts = refs[:groups]
    table, outs, everything = refs[groups], refs[groups + 1 : -1], refs[-1]
    tokens, width = parts[0].shape
    half = width - LANES
    slots = outs[0].shape[0]
    me = lax.axis_index("sp")
    z = lax.axis_index("tp") // 2
    for g in range(groups):
        everything[g * tokens : (g + 1) * tokens, :] = parts[g][...]
    ticket = everything[:, half:].astype(f32)
    lane = lax.broadcasted_iota(jnp.int32, ticket.shape, 1)
    row = lax.broadcasted_iota(jnp.int32, ticket.shape, 0)
    route = [ticket[:, j : j + 1].astype(jnp.int32) for j in range(TOPK)]
    named = me ^ lane
    hit = ((route[0] == named) | (route[1] == named)) & (lane < sp)
    rank = dot(lower[...], hit.astype(f32).astype(bf16)).astype(jnp.int32)
    slot = jnp.where(hit, rank + (z ^ (row // tokens)) * cap, -1)
    named = me ^ (lane // 3)
    tail = jnp.zeros(ticket.shape, f32)
    for j in range(TOPK):
        at = TOPK + 3 * j
        piece = jnp.where(
            lane % 3 == 0,
            ticket[:, at : at + 1],
            jnp.where(lane % 3 == 1, ticket[:, at + 1 : at + 2], ticket[:, at + 2 : at + 3]),
        )
        tail = tail + jnp.where((route[j] == named) & (lane < 3 * sp), piece, 0.0)
    everything[:, half:] = tail.astype(bf16)
    place = lax.broadcasted_iota(jnp.int32, (groups * tokens, slots), 1)
    for k, out in enumerate(outs):
        chosen = (slot[:, k : k + 1] == place).astype(f32).astype(bf16)
        table[k] = chosen
        out[...] = dot_rows(chosen, everything[...]).astype(bf16)


def residual_second_kernel(groups, table, *refs):
    parts = refs[:groups]
    outs, everything = refs[groups:-1], refs[-1]
    tokens = parts[0].shape[0]
    for g in range(groups):
        everything[g * tokens : (g + 1) * tokens, :] = parts[g][...]
    for k, out in enumerate(outs):
        out[...] = dot_rows(table[k], everything[...]).astype(bf16)


def choose_kernel(groups, tokens, gain, table, *refs):
    pieces = refs[: 2 * groups]
    outs = refs[2 * groups : -3]
    own, rows_ref, normed_ref = refs[-3:]
    place = lax.axis_index("tp")
    z, core = place // 2, place % 2
    width = 2 * pieces[0].shape[1]
    for g in range(groups):
        mine, other = pieces[2 * g][...].astype(f32), pieces[2 * g + 1][...].astype(f32)
        first = jnp.where(core == 0, mine, other)
        second = jnp.where(core == 0, other, mine)
        at = pl.multiple_of((z ^ g) * width, width)
        rows_ref[:, pl.ds(at, width)] = jnp.concatenate([first, second], axis=1)
    x = rows_ref[...]
    scale = lax.rsqrt(jnp.mean(x * x, axis=-1, keepdims=True) + epsilon)
    normed_ref[...] = (x * scale * gain[...]).astype(bf16)
    blocks = [
        normed_ref[pl.ds(pl.multiple_of((z ^ g) * tokens, tokens), tokens), :]
        for g in range(groups)
    ]
    own[...] = blocks[0]
    near = jnp.concatenate(blocks, axis=0)
    for k, out in enumerate(outs):
        out[...] = dot_rows(table[k], near).astype(bf16)


def expert_kernel(
    part, chunks, own, out_weight, ffn_gain, gate_a, up_a, down_a, gate_b, up_b, down_b, *refs
):
    count = len(part)
    resids, seconds, norms = refs[:count], refs[count : 2 * count], refs[2 * count : 3 * count]
    outs = refs[-count * chunks - (1 if own else 0) :]
    slots = resids[0].shape[0]
    total = count * slots
    half = seconds[0].shape[1]
    resid_rows = [jnp.concatenate([r[:, :half], t[...]], axis=1) for r, t in zip(resids, seconds)]
    norm_rows = [n[...] for n in norms]
    if own:
        resid_rows.append(refs[3 * count][...])
        norm_rows.append(refs[3 * count + 1][...])
    join = lambda parts: parts[0] if len(parts) == 1 else jnp.concatenate(parts)
    middle = join(resid_rows).astype(f32) + dot(join(norm_rows), out_weight[...])
    if own:
        outs[-1][...] = middle[total:]
        middle = middle[:total]
    scale = lax.rsqrt(jnp.mean(middle * middle, axis=-1, keepdims=True) + epsilon)
    x = (middle * scale * ffn_gain[...]).astype(bf16)
    hiddens = []
    for gate, up in ((gate_a, up_a), (gate_b, up_b)):
        g = dot(x, gate[0])
        u = dot(x, up[0])
        hiddens.append((g / (1.0 + jnp.exp(-g)) * u).astype(bf16))
    shares = []
    for k, r in zip(part, resids):
        tail = r[:, half:].astype(f32)
        lane = lax.broadcasted_iota(jnp.int32, tail.shape, 1)
        shares.append(jnp.sum(jnp.where(lane // 3 == k, tail, 0.0), axis=-1, keepdims=True))
    weight = join(shares)
    chunk = outs[0].shape[1]
    for j in range(chunks):
        cols = slice(j * chunk, (j + 1) * chunk)
        out = dot(hiddens[0], down_a[0, :, cols]) + dot(hiddens[1], down_b[0, :, cols])
        out = (out * weight).astype(bf16)
        for i in range(count):
            outs[i * chunks + j][...] = out[i * slots : (i + 1) * slots]


def combine_kernel(sources, tokens, table, *refs):
    rows, outs = refs[:sources], refs[sources:]
    total = None
    for k in range(sources):
        part = dot(table[k], rows[k][...])
        total = part if total is None else total + part
    for g, out in enumerate(outs):
        out[...] = total[g * tokens : (g + 1) * tokens].astype(out.dtype)


VM = pl.BlockSpec(memory_space=pltpu.VMEM)
ANY = pl.BlockSpec(memory_space=pl.ANY)


def call(body, args, outs, scratch=(), after=(), flops=0, trans=0, inside=(), room=32):
    size = lambda a: int(np.prod(a.shape)) * a.dtype.itemsize
    count = len(args)
    after = list(after)

    def kernel(*refs):
        body(*refs[:count], *refs[count + len(after) :])

    held = [
        pltpu.with_memory_space_constraint(a, pltpu.VMEM) if i in inside else a
        for i, a in enumerate(args)
    ]
    return pl.pallas_call(
        kernel,
        out_shape=outs,
        in_specs=[VM] * count + [ANY] * len(after),
        out_specs=jax.tree.map(lambda _: VM, outs),
        scratch_shapes=list(scratch),
        cost_estimate=pl.CostEstimate(
            flops=int(flops),
            transcendentals=int(trans),
            bytes_accessed=sum(map(size, args)) + sum(map(size, jax.tree.leaves(outs))),
        ),
        compiler_params=pltpu.CompilerParams(vmem_limit_bytes=room * 1024 * 1024),
    )(*held, *after)


def shape(dims, dtype):
    return jax.ShapeDtypeStruct(tuple(dims), dtype)


def program(
    queries, latent, rot_key, latent_gain, key_up, value_up, query_gain, key_gain, out_gain,
    out_weight, residual, ffn_gain, routes, route_weights, expert_gate, expert_up, expert_down,
):
    rows = queries.shape[0]
    heads = key_up.shape[1] // NOPE
    width = residual.shape[1]
    sp, tp = lax.axis_size("sp"), lax.axis_size("tp")
    groups = tp // 2
    tokens = residual.shape[0]
    all_tokens = groups * tokens
    att_width = out_weight.shape[0]
    cap = max(2, 9 * tokens * TOPK // (8 * sp))
    slots = groups * cap

    def swap(v, axis, k, size):
        return lax.ppermute(v, axis, [(i, i ^ k) for i in range(size)])

    swap_core = lambda v: swap(v, "tp", 1, tp)
    swap_z = lambda v, k: swap(v, "tp", 2 * k, tp)
    swap_sp = lambda v, k: swap(v, "sp", k, sp)

    flags = np.zeros((4 * TOPK, LANES), np.float32)
    flags[np.arange(4 * TOPK), np.arange(4 * TOPK)] = 1.0
    ordinal = np.arange(all_tokens)
    lower = (ordinal[:, None] > ordinal[None, :]) & (
        ordinal[:, None] // tokens == ordinal[None, :] // tokens
    )
    lower = jnp.asarray(lower.astype(np.float32), bf16)
    first_half, second_half = call(
        pack_kernel,
        [routes.T, route_weights.T, residual, jnp.asarray(flags, bf16)],
        (shape((tokens, width // 2 + LANES), bf16), shape((tokens, width // 2), bf16)),
        room=ROOM,
    )
    first_parts = [first_half] + [swap_z(first_half, k) for k in range(1, groups)]
    second_parts = [second_half] + [swap_z(second_half, k) for k in range(1, groups)]

    pack = LANES // (ROPE * heads)
    inner, first = turn_tables(rows, sp)
    selk = jnp.asarray(np.concatenate(rope_select(0, ROPE), axis=1), bf16)
    selq = jnp.asarray(head_select(heads), bf16)
    selg = jnp.asarray(np.abs(head_select(1)), f32)
    bundle, q1, q2 = call(
        functools.partial(prep_kernel, heads),
        [
            latent, rot_key.T, latent_gain[None, :], key_up, value_up, queries.T,
            query_gain[None, :], key_gain[None, :], inner, first, selq, selk, selg,
        ],
        (
            shape((heads * rows + rows // pack, LANES), bf16),
            shape((heads, rows, LANES), bf16),
            shape((heads * pack, rows, LANES), bf16),
        ),
        flops=2 * rows * latent.shape[1] * 256 + 2 * rows * 192 * 768,
        room=ROOM,
    )
    bundles = [bundle] + [swap_sp(bundle, k) for k in range(1, sp)]

    gate_b = swap_core(expert_gate)
    up_b = swap_core(expert_up)
    down_b = swap_core(expert_down)
    table, *first_rows = call(
        functools.partial(residual_first_kernel, groups, sp, cap),
        [lower] + first_parts,
        (shape((sp, all_tokens, slots), bf16),)
        + tuple([shape((slots, width // 2 + LANES), bf16)] * sp),
        [pltpu.VMEM((all_tokens, width // 2 + LANES), bf16)],
        flops=sp * slots * all_tokens * width,
    )
    first_in = [first_rows[0]] + [swap_sp(first_rows[k], k) for k in range(1, sp)]

    half = heads * VH
    split = min(3, sp)
    early, late = list(range(split)), list(range(split, sp))
    state = call(
        functools.partial(attend_first_kernel, heads, early),
        [q1, q2] + [bundles[k] for k in early],
        shape((heads, LANES, rows), f32),
        room=ROOM,
        flops=2 * heads * rows * rows * len(early) * 384,
        trans=heads * rows * rows * len(early),
    )
    keep, send = call(
        functools.partial(attend_last_kernel, heads, tokens, groups, late),
        [q1, q2, state] + [bundles[k] for k in late],
        (shape((all_tokens, half), bf16), shape((all_tokens, half), bf16)),
        [pltpu.VMEM((heads, LANES, rows), f32), pltpu.VMEM((rows, half), f32)],
        room=ROOM,
        flops=2 * heads * rows * rows * len(late) * 384,
        trans=heads * rows * rows * len(late),
    )
    second_rows = call(
        functools.partial(residual_second_kernel, groups),
        [table] + second_parts,
        tuple([shape((slots, width // 2), bf16)] * sp),
        [pltpu.VMEM((all_tokens, width // 2), bf16)],
        flops=sp * slots * all_tokens * width,
    )
    second_in = [second_rows[0]] + [swap_sp(second_rows[k], k) for k in range(1, sp)]
    other = swap_core(send)
    pieces = [keep, other]
    kept_in = [swap_z(keep, k) for k in range(1, groups)]
    other_in = [swap_z(other, k) for k in range(1, groups)]
    for a, b in zip(kept_in, other_in):
        pieces += [a, b]
    *norm_rows, own_rows = call(
        functools.partial(choose_kernel, groups, tokens),
        [out_gain[None, :], table] + pieces,
        tuple([shape((slots, att_width), bf16)] * sp) + (shape((tokens, att_width), bf16),),
        [pltpu.VMEM((all_tokens, att_width), f32), pltpu.VMEM((all_tokens, att_width), bf16)],
        flops=2 * sp * slots * all_tokens * att_width,
    )
    norm_in = [norm_rows[0]] + [swap_sp(norm_rows[k], k) for k in range(1, sp)]

    hidden = 2 * expert_gate.shape[2]
    chunk = width // COL_CHUNKS
    parts = expert_parts(sp)
    served = [None] * sp
    before = []
    for n, part in enumerate(parts):
        extra_in = [residual, own_rows] if n == 0 else []
        extra_out = (shape((tokens, width), f32),) if n == 0 else ()
        outs = call(
            functools.partial(expert_kernel, part, COL_CHUNKS, n == 0),
            [
                out_weight, ffn_gain[None, :], expert_gate, expert_up, expert_down,
                gate_b, up_b, down_b,
            ]
            + [first_in[k] for k in part]
            + [second_in[k] for k in part]
            + [norm_in[k] for k in part]
            + extra_in,
            tuple([shape((slots, chunk), bf16)] * (len(part) * COL_CHUNKS)) + extra_out,
            after=before,
            flops=2 * len(part) * slots * width * (att_width + 3 * hidden),
            inside=(0, 2, 3, 4, 5, 6, 7),
        )
        if n == 0:
            middle = outs[-1]
        before = [outs[0]]
        for i, k in enumerate(part):
            served[k] = outs[i * COL_CHUNKS : (i + 1) * COL_CHUNKS]
    finished = []
    for j in range(COL_CHUNKS):
        back = [served[0][j]] + [swap_sp(served[k][j], k) for k in range(1, sp)]
        own, *rest = call(
            functools.partial(combine_kernel, sp, tokens),
            [table] + back,
            (shape((tokens, chunk), f32),) + tuple([shape((tokens, chunk), bf16)] * (groups - 1)),
            flops=2 * all_tokens * sp * slots * chunk,
        )
        total = middle[:, j * chunk : (j + 1) * chunk] + own
        for k in range(1, groups):
            total = total + swap_z(rest[k - 1], k).astype(f32)
        finished.append(total.astype(bf16))
    return jnp.concatenate(finished, axis=1)


def expert_parts(sp):
    parts, at = [[0], [k for k in (1, 2) if k < sp]], 3
    while at < sp:
        parts.append(list(range(at, min(at + 4, sp))))
        at += 4
    return [p for p in parts if p]


def solution(mesh):
    return jax.shard_map(
        program,
        mesh=mesh,
        in_specs=(
            P("sp", "tp"),
            P("sp", None),
            P("sp", None),
            P(),
            P(None, "tp"),
            P(None, "tp"),
            P(),
            P(),
            P(),
            P(),
            P(("sp", "tp"), None),
            P(),
            P(("sp", "tp"), None),
            P(("sp", "tp"), None),
            P("sp", None, "tp"),
            P("sp", None, "tp"),
            P("sp", "tp", None),
        ),
        out_specs=P(("sp", "tp"), None),
        check_vma=False,
    )
```

```python
import functools

import jax
import jax.numpy as jnp
import numpy as np
from jax import lax
from jax.experimental import pallas as pl
from jax.experimental.pallas import tpu as pltpu
from jax.sharding import PartitionSpec as P


NOPE = 64
ROPE = 32
VH = 64
TOPK = 2
QK = 96
LANES = 128
COL_CHUNKS = 2
APART = 4
ROOM = 60
ATTEND_ROOM = 44


epsilon = 1e-06
rope_base = 10000.0
f32 = jnp.float32
bf16 = jnp.bfloat16


def dot(a, b):
    return jnp.dot(a, b, preferred_element_type=f32)


def rope_select(offset, rows):
    direct = np.zeros((rows, LANES), np.float32)
    turned = np.zeros((rows, LANES), np.float32)
    half = ROPE // 2
    for lane in range(LANES):
        d = lane % ROPE
        direct[offset + d, lane] = 1.0
        turned[offset + (d + half) % ROPE, lane] = -1.0 if d < half else 1.0
    return direct, turned


def head_select(heads):
    parts = []
    for h in range(heads):
        nope = np.zeros((heads * QK, LANES), np.float32)
        for i in range(NOPE):
            nope[h * QK + i, i] = 1.0
        parts += [nope, *rope_select(h * QK + NOPE, heads * QK)]
    return np.concatenate(parts, axis=1)


def turn_tables(rows, blocks):
    inverse = rope_base ** (-np.arange(0, ROPE, 2, dtype=np.float64) / ROPE)
    inverse = np.tile(inverse, 2 * LANES // ROPE)[None, :]
    inner = np.arange(rows, dtype=np.float64)[:, None] * inverse
    first = np.arange(blocks, dtype=np.float64)[:, None] * rows * inverse
    return [
        np.concatenate([np.cos(a), np.sin(a)], axis=1).astype(np.float32) for a in (inner, first)
    ]


def dot_rows(a, b):
    return lax.dot_general(a, b, (((0,), (0,)), ((), ())), preferred_element_type=f32)


def prep_kernel(
    heads, lat, rot, lat_gain, key_up, value_up, queries, q_gain, k_gain, inner, first,
    selq, selk, selg, routes, route_weights, residual, flags, bundle, q1, q2, head, rest,
):
    pack_rows(routes, route_weights, residual, flags, head, rest)
    rows = lat.shape[0]
    pack = LANES // (ROPE * heads)
    sub = rows // pack
    me = lax.axis_index("sp")
    x = lat[...].astype(f32)
    scale = lax.rsqrt(jnp.mean(x * x, axis=-1, keepdims=True) + epsilon)
    normed = (x * scale * lat_gain[...]).astype(bf16)
    base = first[pl.ds(me, 1), :]
    base_cos, base_sin = base[:, :LANES], base[:, LANES:]
    in_cos, in_sin = inner[:, :LANES], inner[:, LANES:]
    cos = in_cos * base_cos - in_sin * base_sin
    sin = in_sin * base_cos + in_cos * base_sin
    spread_gain = lambda g: jnp.dot(
        g[...], selg[...], precision=lax.Precision.HIGHEST, preferred_element_type=f32
    )
    gq, gk = spread_gain(q_gain), spread_gain(k_gain)
    cut = lambda g, i: g[:, i * LANES : (i + 1) * LANES]
    lane = lax.broadcasted_iota(jnp.int32, (rows, LANES), 1)
    is_key = lane < NOPE
    turns = dot_rows(rot[...], selk[...])
    rot_a, rot_b = turns[:, :LANES], turns[:, LANES:]
    rot_sq = jnp.sum(rot_a * rot_a, axis=-1, keepdims=True) * (ROPE / LANES)
    spun = rot_a * cut(gk, 1) * cos + rot_b * cut(gk, 2) * sin
    key_scales = None
    for h in range(heads):
        weight = jnp.concatenate(
            [key_up[:, h * NOPE : (h + 1) * NOPE], value_up[:, h * VH : (h + 1) * VH]], axis=1
        )
        kv = dot(normed, weight).astype(bf16).astype(f32)
        sq = jnp.sum(jnp.where(is_key, kv * kv, 0.0), axis=-1, keepdims=True) + rot_sq
        r = lax.rsqrt(sq * (1.0 / QK) + epsilon)
        bundle[h * rows : (h + 1) * rows, :] = jnp.where(
            is_key, kv * r * cut(gk, 0), kv
        ).astype(bf16)
        spread = jnp.broadcast_to(r, (rows, LANES))
        key_scales = (
            spread
            if key_scales is None
            else jnp.where((lane // ROPE) % heads == h, spread, key_scales)
        )
    spun = spun * key_scales
    tile = spun[:sub]
    for p in range(1, pack):
        tile = jnp.where(
            lane[:sub] // (ROPE * heads) == p, spun[p * sub : (p + 1) * sub], tile
        )
    bundle[heads * rows :, :] = tile.astype(bf16)
    picked = dot_rows(queries[...], selq[...])
    for h in range(heads):
        base = h * 3 * LANES
        nope = picked[:, base : base + LANES]
        qa = picked[:, base + LANES : base + 2 * LANES]
        qb = picked[:, base + 2 * LANES : base + 3 * LANES]
        sq = jnp.sum(nope * nope + qa * qa * (ROPE / LANES), axis=-1, keepdims=True)
        r = lax.rsqrt(sq * (1.0 / QK) + epsilon)
        q1[h] = (nope * r * cut(gq, 0)).astype(bf16)
        turned = (qa * cut(gq, 1) * cos + qb * cut(gq, 2) * sin) * r
        for p in range(pack):
            q2[h * pack + p] = jnp.where(lane // ROPE == p * heads + h, turned, 0.0).astype(bf16)


def scores_of(heads, q1, q2, ref, h, top, count, parts):
    rows = q1.shape[1]
    pack = LANES // (ROPE * heads)
    sub = rows // pack
    out = []
    for p in range(parts):
        query = jnp.concatenate(
            [q1[h, top : top + count], q2[h * pack + p, top : top + count]], axis=1
        )
        key = jnp.concatenate(
            [
                ref[h * rows + p * sub : h * rows + (p + 1) * sub, :],
                ref[heads * rows : heads * rows + sub, :],
            ],
            axis=1,
        )
        out.append(
            lax.dot_general(key, query, (((1,), (1,)), ((), ())), preferred_element_type=f32)
        )
    return out[0] if parts == 1 else jnp.concatenate(out, axis=0)


FACTOR = float(QK ** (-0.5) * np.log2(np.e))


def attend_own(heads, q1, q2, ref, state):
    rows = q1.shape[1]
    pack = LANES // (ROPE * heads)
    sub = rows // pack
    for h in range(heads):
        for b in range(pack):
            scores = scores_of(heads, q1, q2, ref, h, b * sub, sub, b + 1)
            key = lax.broadcasted_iota(jnp.int32, scores.shape, 0)
            query = lax.broadcasted_iota(jnp.int32, scores.shape, 1) + b * sub
            scores = jnp.where(key <= query, scores, -1e30)
            peak = jnp.max(scores, axis=0, keepdims=True)
            weights = jnp.exp2((scores - peak) * FACTOR)
            total = jnp.sum(weights, axis=0, keepdims=True)
            part = dot_rows(ref[h * rows : h * rows + (b + 1) * sub, :], weights.astype(bf16))
            row = lax.broadcasted_iota(jnp.int32, part.shape, 0)
            state[h, :, b * sub : (b + 1) * sub] = jnp.where(
                row == 0, peak, jnp.where(row == 1, total, part)
            )


def attend_other(heads, q1, q2, ref, state):
    rows = q1.shape[1]
    pack = LANES // (ROPE * heads)
    for h in range(heads):
        scores = scores_of(heads, q1, q2, ref, h, 0, rows, pack)
        old = state[h, 0:1, :]
        peak = jnp.maximum(old, jnp.max(scores, axis=0, keepdims=True))
        fade = jnp.exp2((old - peak) * FACTOR)
        weights = jnp.exp2((scores - peak) * FACTOR)
        total = state[h, 1:2, :] * fade + jnp.sum(weights, axis=0, keepdims=True)
        part = dot_rows(ref[h * rows : (h + 1) * rows, :], weights.astype(bf16))
        part = part + state[h] * fade
        row = lax.broadcasted_iota(jnp.int32, part.shape, 0)
        state[h] = jnp.where(row == 0, peak, jnp.where(row == 1, total, part))


def attend_kernel(heads, tokens, groups, q1, q2, *refs):
    bundles = refs[:-4]
    keep, send, state, result = refs[-4:]
    me = lax.axis_index("sp")
    core = lax.axis_index("tp") % 2
    attend_own(heads, q1, q2, bundles[0], state)
    for k in range(1, len(bundles)):

        @pl.when((me ^ k) < me)
        def _():
            attend_other(heads, q1, q2, bundles[k], state)

    outs = [state[h, NOPE:, :] / state[h, 1:2, :] for h in range(heads)]
    result[...] = (outs[0] if heads == 1 else jnp.concatenate(outs, axis=0)).T
    for g in range(groups):
        at = g * 2 * tokens
        keep[g * tokens : (g + 1) * tokens, :] = result[
            pl.ds(pl.multiple_of(at + core * tokens, tokens), tokens), :
        ].astype(bf16)
        send[g * tokens : (g + 1) * tokens, :] = result[
            pl.ds(pl.multiple_of(at + (1 - core) * tokens, tokens), tokens), :
        ].astype(bf16)


def pack_rows(routes, weights, residual, flags, first, second):
    half = second.shape[1]
    rows = [routes[...].astype(f32)]
    for j in range(TOPK):
        rest = weights[j : j + 1, :]
        for _ in range(3):
            piece = rest.astype(bf16).astype(f32)
            rows.append(piece)
            rest = rest - piece
    stacked = jnp.concatenate(rows, axis=0)
    first[:, :half] = residual[:, :half]
    first[:, half:] = dot_rows(stacked.astype(bf16), flags[...]).astype(bf16)
    second[...] = residual[:, half:]


def residual_first_kernel(groups, sp, cap, lower, *refs):
    parts = refs[:groups]
    table, outs, everything = refs[groups], refs[groups + 1 : -1], refs[-1]
    tokens, width = parts[0].shape
    half = width - LANES
    slots = outs[0].shape[0]
    me = lax.axis_index("sp")
    for g in range(groups):
        everything[g * tokens : (g + 1) * tokens, :] = parts[g][...]
    ticket = everything[:, half:].astype(f32)
    lane = lax.broadcasted_iota(jnp.int32, ticket.shape, 1)
    row = lax.broadcasted_iota(jnp.int32, ticket.shape, 0)
    route = [ticket[:, j : j + 1].astype(jnp.int32) for j in range(TOPK)]
    named = me ^ lane
    hit = ((route[0] == named) | (route[1] == named)) & (lane < sp)
    rank = dot(lower[...], hit.astype(f32).astype(bf16)).astype(jnp.int32)
    slot = jnp.where(hit, rank + (row // tokens) * cap, -1)
    named = me ^ (lane // 3)
    tail = jnp.zeros(ticket.shape, f32)
    for j in range(TOPK):
        at = TOPK + 3 * j
        piece = jnp.where(
            lane % 3 == 0,
            ticket[:, at : at + 1],
            jnp.where(lane % 3 == 1, ticket[:, at + 1 : at + 2], ticket[:, at + 2 : at + 3]),
        )
        tail = tail + jnp.where((route[j] == named) & (lane < 3 * sp), piece, 0.0)
    everything[:, half:] = tail.astype(bf16)
    place = lax.broadcasted_iota(jnp.int32, (groups * tokens, slots), 1)
    for k, out in enumerate(outs):
        chosen = (slot[:, k : k + 1] == place).astype(f32).astype(bf16)
        table[k] = chosen
        out[...] = dot_rows(chosen, everything[...]).astype(bf16)


def residual_second_kernel(groups, table, *refs):
    parts = refs[:groups]
    outs, everything = refs[groups:-1], refs[-1]
    tokens = parts[0].shape[0]
    for g in range(groups):
        everything[g * tokens : (g + 1) * tokens, :] = parts[g][...]
    for k, out in enumerate(outs):
        out[...] = dot_rows(table[k], everything[...]).astype(bf16)


def choose_kernel(groups, tokens, gain, table, *refs):
    pieces = refs[: 2 * groups]
    outs = refs[2 * groups : -3]
    own, rows_ref, normed_ref = refs[-3:]
    place = lax.axis_index("tp")
    z, core = place // 2, place % 2
    width = 2 * pieces[0].shape[1]
    for g in range(groups):
        mine, other = pieces[2 * g][...].astype(f32), pieces[2 * g + 1][...].astype(f32)
        first = jnp.where(core == 0, mine, other)
        second = jnp.where(core == 0, other, mine)
        at = pl.multiple_of((z ^ g) * width, width)
        rows_ref[:, pl.ds(at, width)] = jnp.concatenate([first, second], axis=1)
    x = rows_ref[...]
    scale = lax.rsqrt(jnp.mean(x * x, axis=-1, keepdims=True) + epsilon)
    normed_ref[...] = (x * scale * gain[...]).astype(bf16)
    blocks = [
        normed_ref[pl.ds(pl.multiple_of((z ^ g) * tokens, tokens), tokens), :]
        for g in range(groups)
    ]
    own[...] = blocks[0]
    near = jnp.concatenate(blocks, axis=0)
    for k, out in enumerate(outs):
        out[...] = dot_rows(table[k], near).astype(bf16)


def expert_kernel(
    part, chunks, own, cap, carried, out_weight, ffn_gain, gate_a, up_a, down_a, gate_b, up_b, down_b, *refs
):
    count = len(part)
    resids, seconds, norms = refs[:count], refs[count : 2 * count], refs[2 * count : 3 * count]
    slots = resids[0].shape[0]
    groups = slots // cap
    results = count * chunks + groups + (1 if own else 0)
    outs, apart = refs[-results:], refs[-results:][count * chunks :][:groups]
    brought = refs[-results - groups : -results] if carried else ()
    total = count * slots
    half = seconds[0].shape[1]
    resid_rows = [jnp.concatenate([r[:, :half], t[...]], axis=1) for r, t in zip(resids, seconds)]
    norm_rows = [n[...] for n in norms]
    if own:
        resid_rows.append(refs[3 * count][...])
        norm_rows.append(refs[3 * count + 1][...])
    join = lambda parts: parts[0] if len(parts) == 1 else jnp.concatenate(parts)
    middle = join(resid_rows).astype(f32) + dot(join(norm_rows), out_weight[...])
    if own:
        outs[-1][...] = middle[total:]
        middle = middle[:total]
    scale = lax.rsqrt(jnp.mean(middle * middle, axis=-1, keepdims=True) + epsilon)
    x = (middle * scale * ffn_gain[...]).astype(bf16)
    hiddens = []
    for gate, up in ((gate_a, up_a), (gate_b, up_b)):
        g = dot(x, gate[0])
        u = dot(x, up[0])
        hiddens.append((g / (1.0 + jnp.exp(-g)) * u).astype(bf16))
    shares = []
    for k, r in zip(part, resids):
        tail = r[:, half:].astype(f32)
        lane = lax.broadcasted_iota(jnp.int32, tail.shape, 1)
        shares.append(jnp.sum(jnp.where(lane // 3 == k, tail, 0.0), axis=-1, keepdims=True))
    weight = join(shares)
    chunk = outs[0].shape[1]
    for j in range(chunks):
        cols = slice(j * chunk, (j + 1) * chunk)
        out = dot(hiddens[0], down_a[0, :, cols]) + dot(hiddens[1], down_b[0, :, cols])
        out = (out * weight).astype(bf16)
        for i in range(count):
            outs[i * chunks + j][...] = out[i * slots : (i + 1) * slots]
    out = dot(hiddens[0], down_a[0, :, chunks * chunk :])
    out = (out + dot(hiddens[1], down_b[0, :, chunks * chunk :])) * weight
    for g in range(groups):
        pieces = [out[i * slots + g * cap : i * slots + (g + 1) * cap] for i in range(count)]
        if carried:
            pieces = [brought[g][...].astype(f32)] + pieces
        apart[g][...] = join(pieces).astype(bf16)


def sum_kernel(groups, cap, *refs):
    parts, outs = refs[:groups], refs[groups:]
    total = parts[0][...].astype(f32)
    for part in parts[1:]:
        total = total + part[...].astype(f32)
    for i, out in enumerate(outs):
        out[...] = total[i * cap : (i + 1) * cap].astype(bf16)


def finish_kernel(sp, tokens, cap, table, middle, *refs):
    rows, out = refs[:sp], refs[sp]
    width = out.shape[1]
    total = middle[:, middle.shape[1] - width :]
    for k in range(sp):
        total = total + dot(table[k, :tokens, :cap], rows[k][...])
    out[...] = total.astype(bf16)


def combine_kernel(sources, tokens, place, chunk, table, *refs):
    rows, outs = refs[:sources], refs[sources:]
    total = None
    for k in range(sources):
        at = 0 if rows[k].shape[1] == chunk else place * chunk
        part = dot(table[k], rows[k][:, at : at + chunk])
        total = part if total is None else total + part
    for g, out in enumerate(outs):
        out[...] = total[g * tokens : (g + 1) * tokens].astype(out.dtype)


VM = pl.BlockSpec(memory_space=pltpu.VMEM)
ANY = pl.BlockSpec(memory_space=pl.ANY)


def call(body, args, outs, scratch=(), after=(), flops=0, trans=0, room=32):
    size = lambda a: int(np.prod(a.shape)) * a.dtype.itemsize
    count = len(args)
    after = list(after)

    def kernel(*refs):
        body(*refs[:count], *refs[count + len(after) :])

    return pl.pallas_call(
        kernel,
        out_shape=outs,
        in_specs=[VM] * count + [ANY] * len(after),
        out_specs=jax.tree.map(lambda _: VM, outs),
        scratch_shapes=list(scratch),
        cost_estimate=pl.CostEstimate(
            flops=int(flops),
            transcendentals=int(trans),
            bytes_accessed=sum(map(size, args)) + sum(map(size, jax.tree.leaves(outs))),
        ),
        compiler_params=pltpu.CompilerParams(vmem_limit_bytes=room * 1024 * 1024),
    )(*args, *after)


def shape(dims, dtype):
    return jax.ShapeDtypeStruct(tuple(dims), dtype)


def program(
    queries, latent, rot_key, latent_gain, key_up, value_up, query_gain, key_gain, out_gain,
    out_weight, residual, ffn_gain, routes, route_weights, expert_gate, expert_up, expert_down,
):
    rows = queries.shape[0]
    heads = key_up.shape[1] // NOPE
    width = residual.shape[1]
    sp, tp = lax.axis_size("sp"), lax.axis_size("tp")
    groups = tp // 2
    tokens = residual.shape[0]
    all_tokens = groups * tokens
    att_width = out_weight.shape[0]
    cap = max(2, 9 * tokens * TOPK // (8 * sp))
    slots = groups * cap

    def swap(v, axis, k, size):
        return lax.ppermute(v, axis, [(i, i ^ k) for i in range(size)])

    def gather_z(v):
        return [v] + [swap_z(v, k) for k in range(1, groups)]

    swap_core = lambda v: swap(v, "tp", 1, tp)
    swap_z = lambda v, k: swap(v, "tp", 2 * k, tp)
    swap_sp = lambda v, k: swap(v, "sp", k, sp)

    flags = np.zeros((4 * TOPK, LANES), np.float32)
    flags[np.arange(4 * TOPK), np.arange(4 * TOPK)] = 1.0
    ordinal = np.arange(all_tokens)
    lower = (ordinal[:, None] > ordinal[None, :]) & (
        ordinal[:, None] // tokens == ordinal[None, :] // tokens
    )
    lower = jnp.asarray(lower.astype(np.float32), bf16)
    pack = LANES // (ROPE * heads)
    inner, first = turn_tables(rows, sp)
    selk = jnp.asarray(np.concatenate(rope_select(0, ROPE), axis=1), bf16)
    selq = jnp.asarray(head_select(heads), bf16)
    selg = jnp.asarray(np.abs(head_select(1)), f32)
    bundle, q1, q2, first_half, second_half = call(
        functools.partial(prep_kernel, heads),
        [
            latent, rot_key.T, latent_gain[None, :], key_up, value_up, queries.T,
            query_gain[None, :], key_gain[None, :], inner, first, selq, selk, selg,
            routes.T, route_weights.T, residual, jnp.asarray(flags, bf16),
        ],
        (
            shape((heads * rows + rows // pack, LANES), bf16),
            shape((heads, rows, LANES), bf16),
            shape((heads * pack, rows, LANES), bf16),
            shape((tokens, width // 2 + LANES), bf16),
            shape((tokens, width // 2), bf16),
        ),
        flops=2 * rows * latent.shape[1] * 256 + 2 * rows * 192 * 768,
        room=ROOM,
    )
    first_parts = gather_z(first_half)
    second_parts = gather_z(second_half)
    bundles = [bundle] + [swap_sp(bundle, k) for k in range(1, sp)]

    gate_b = swap_core(expert_gate)
    up_b = swap_core(expert_up)
    down_b = swap_core(expert_down)
    table, *first_rows = call(
        functools.partial(residual_first_kernel, groups, sp, cap),
        [lower] + first_parts,
        (shape((sp, all_tokens, slots), bf16),)
        + tuple([shape((slots, width // 2 + LANES), bf16)] * sp),
        [pltpu.VMEM((all_tokens, width // 2 + LANES), bf16)],
        flops=sp * slots * all_tokens * width,
    )
    first_in = [first_rows[0]] + [swap_sp(first_rows[k], k) for k in range(1, sp)]

    half = heads * VH
    keep, send = call(
        functools.partial(attend_kernel, heads, tokens, groups),
        [q1, q2] + bundles,
        (shape((all_tokens, half), bf16), shape((all_tokens, half), bf16)),
        [pltpu.VMEM((heads, LANES, rows), f32), pltpu.VMEM((rows, half), f32)],
        room=ATTEND_ROOM,
        flops=2 * heads * rows * rows * sp * 384,
        trans=heads * rows * rows * sp,
    )
    second_rows = call(
        functools.partial(residual_second_kernel, groups),
        [table] + second_parts,
        tuple([shape((slots, width // 2), bf16)] * sp),
        [pltpu.VMEM((all_tokens, width // 2), bf16)],
        flops=sp * slots * all_tokens * width,
    )
    second_in = [second_rows[0]] + [swap_sp(second_rows[k], k) for k in range(1, sp)]
    other = swap_core(send)
    pieces = []
    for pair in zip(gather_z(keep), gather_z(other)):
        pieces += pair
    *norm_rows, own_rows = call(
        functools.partial(choose_kernel, groups, tokens),
        [out_gain[None, :], table] + pieces,
        tuple([shape((slots, att_width), bf16)] * sp) + (shape((tokens, att_width), bf16),),
        [pltpu.VMEM((all_tokens, att_width), f32), pltpu.VMEM((all_tokens, att_width), bf16)],
        flops=2 * sp * slots * all_tokens * att_width,
    )
    norm_in = [norm_rows[0]] + [swap_sp(norm_rows[k], k) for k in range(1, sp)]

    hidden = 2 * expert_gate.shape[2]
    apart = width // APART
    chunk = (width - apart) // COL_CHUNKS
    parts = expert_parts(sp)
    served, summed = [None] * sp, [None] * sp
    before, carried = [], []
    for n, part in enumerate(parts):
        own, last = n == 0, n == len(parts) - 1
        extra_in = ([residual, own_rows] if own else []) + (carried if last and n else [])
        extra_out = (shape((tokens, width), f32),) if own else ()
        members = ([0] if last and n else []) + part
        cuts = COL_CHUNKS if last else 1
        outs = call(
            functools.partial(expert_kernel, part, cuts, own, cap, bool(last and n)),
            [
                out_weight, ffn_gain[None, :], expert_gate, expert_up, expert_down,
                gate_b, up_b, down_b,
            ]
            + [first_in[k] for k in part]
            + [second_in[k] for k in part]
            + [norm_in[k] for k in part]
            + extra_in,
            tuple([shape((slots, chunk * COL_CHUNKS // cuts), bf16)] * (len(part) * cuts))
            + tuple([shape((len(members) * cap, apart), bf16)] * groups)
            + extra_out,
            after=before,
            flops=2 * len(part) * slots * width * (att_width + 3 * hidden),
        )
        before = [outs[0]]
        for i, k in enumerate(part):
            served[k] = [swap_sp(v, k) if k else v for v in outs[i * cuts : (i + 1) * cuts]]
        split = outs[len(part) * cuts :][:groups]
        if own:
            middle = outs[-1]
            carried = list(split)
        if not own or last:
            sums = call(
                functools.partial(sum_kernel, groups, cap),
                [split[0]] + [swap_z(split[k], k) for k in range(1, groups)],
                tuple([shape((cap, apart), bf16)] * len(members)),
            )
            for k, v in zip(members, sums):
                summed[k] = swap_sp(v, k) if k else v
    finished = []
    for j in range(COL_CHUNKS):
        back = [v[min(j, len(v) - 1)] for v in served]
        own, *rest = call(
            functools.partial(combine_kernel, sp, tokens, j, chunk),
            [table] + back,
            (shape((tokens, chunk), f32),) + tuple([shape((tokens, chunk), bf16)] * (groups - 1)),
            flops=2 * all_tokens * sp * slots * chunk,
        )
        total = middle[:, j * chunk : (j + 1) * chunk] + own
        for k in range(1, groups):
            total = total + swap_z(rest[k - 1], k).astype(f32)
        finished.append(total.astype(bf16))
    finished.append(
        call(
            functools.partial(finish_kernel, sp, tokens, cap),
            [table, middle] + summed,
            shape((tokens, apart), bf16),
        )
    )
    return jnp.concatenate(finished, axis=1)


def expert_parts(sp):
    parts, at = [[0], [k for k in (1, 2) if k < sp]], 3
    while at < sp:
        parts.append(list(range(at, min(at + 4, sp))))
        at += 4
    return [p for p in parts if p]


def solution(mesh):
    return jax.shard_map(
        program,
        mesh=mesh,
        in_specs=(
            P("sp", "tp"),
            P("sp", None),
            P("sp", None),
            P(),
            P(None, "tp"),
            P(None, "tp"),
            P(),
            P(),
            P(),
            P(),
            P(("sp", "tp"), None),
            P(),
            P(("sp", "tp"), None),
            P(("sp", "tp"), None),
            P("sp", None, "tp"),
            P("sp", None, "tp"),
            P("sp", "tp", None),
        ),
        out_specs=P(("sp", "tp"), None),
        check_vma=False,
    )
```

```python
import functools

import jax
import jax.numpy as jnp
import numpy as np
from jax import lax
from jax.experimental import pallas as pl
from jax.experimental.pallas import tpu as pltpu
from jax.sharding import PartitionSpec as P


NOPE = 64
ROPE = 32
VH = 64
TOPK = 2
QK = 96
LANES = 128
COL_CHUNKS = 2
APART = 4
ROOM = 60
ATTEND_ROOM = 44


epsilon = 1e-06
rope_base = 10000.0
f32 = jnp.float32
bf16 = jnp.bfloat16


def dot(a, b):
    return jnp.dot(a, b, preferred_element_type=f32)


def rope_select(offset, rows):
    direct = np.zeros((rows, LANES), np.float32)
    turned = np.zeros((rows, LANES), np.float32)
    half = ROPE // 2
    for lane in range(LANES):
        d = lane % ROPE
        direct[offset + d, lane] = 1.0
        turned[offset + (d + half) % ROPE, lane] = -1.0 if d < half else 1.0
    return direct, turned


def head_select(heads):
    parts = []
    for h in range(heads):
        nope = np.zeros((heads * QK, LANES), np.float32)
        for i in range(NOPE):
            nope[h * QK + i, i] = 1.0
        parts += [nope, *rope_select(h * QK + NOPE, heads * QK)]
    return np.concatenate(parts, axis=1)


def turn_tables(rows, blocks):
    inverse = rope_base ** (-np.arange(0, ROPE, 2, dtype=np.float64) / ROPE)
    inverse = np.tile(inverse, 2 * LANES // ROPE)[None, :]
    inner = np.arange(rows, dtype=np.float64)[:, None] * inverse
    first = np.arange(blocks, dtype=np.float64)[:, None] * rows * inverse
    return [
        np.concatenate([np.cos(a), np.sin(a)], axis=1).astype(np.float32) for a in (inner, first)
    ]


def dot_rows(a, b):
    return lax.dot_general(a, b, (((0,), (0,)), ((), ())), preferred_element_type=f32)


def prep_kernel(
    heads, lat, rot, lat_gain, key_up, value_up, queries, q_gain, k_gain, inner, first,
    selq, selk, selg, routes, route_weights, residual, flags, bundle, q, head, rest,
):
    pack_rows(routes, route_weights, residual, flags, head, rest)
    rows = lat.shape[0]
    pack = LANES // (ROPE * heads)
    sub = rows // pack
    me = lax.axis_index("sp")
    x = lat[...].astype(f32)
    scale = lax.rsqrt(jnp.mean(x * x, axis=-1, keepdims=True) + epsilon)
    normed = (x * scale * lat_gain[...]).astype(bf16)
    base = first[pl.ds(me, 1), :]
    base_cos, base_sin = base[:, :LANES], base[:, LANES:]
    in_cos, in_sin = inner[:, :LANES], inner[:, LANES:]
    cos = in_cos * base_cos - in_sin * base_sin
    sin = in_sin * base_cos + in_cos * base_sin
    spread_gain = lambda g: jnp.dot(
        g[...], selg[...], precision=lax.Precision.HIGHEST, preferred_element_type=f32
    )
    gq, gk = spread_gain(q_gain), spread_gain(k_gain)
    cut = lambda g, i: g[:, i * LANES : (i + 1) * LANES]
    lane = lax.broadcasted_iota(jnp.int32, (rows, LANES), 1)
    is_key = lane < NOPE
    turns = dot_rows(rot[...], selk[...])
    rot_a, rot_b = turns[:, :LANES], turns[:, LANES:]
    rot_sq = jnp.sum(rot_a * rot_a, axis=-1, keepdims=True) * (ROPE / LANES)
    spun = rot_a * cut(gk, 1) * cos + rot_b * cut(gk, 2) * sin
    key_scales = None
    for h in range(heads):
        weight = jnp.concatenate(
            [key_up[:, h * NOPE : (h + 1) * NOPE], value_up[:, h * VH : (h + 1) * VH]], axis=1
        )
        kv = dot(normed, weight).astype(bf16).astype(f32)
        sq = jnp.sum(jnp.where(is_key, kv * kv, 0.0), axis=-1, keepdims=True) + rot_sq
        r = lax.rsqrt(sq * (1.0 / QK) + epsilon)
        bundle[h * rows : (h + 1) * rows, :] = jnp.where(
            is_key, kv * r * cut(gk, 0), kv
        ).astype(bf16)
        spread = jnp.broadcast_to(r, (rows, LANES))
        key_scales = (
            spread
            if key_scales is None
            else jnp.where((lane // ROPE) % heads == h, spread, key_scales)
        )
    spun = spun * key_scales
    tile = spun[:sub]
    for p in range(1, pack):
        tile = jnp.where(
            lane[:sub] // (ROPE * heads) == p, spun[p * sub : (p + 1) * sub], tile
        )
    bundle[heads * rows :, :] = tile.astype(bf16)
    picked = dot_rows(queries[...], selq[...])
    for h in range(heads):
        base = h * 3 * LANES
        nope = picked[:, base : base + LANES]
        qa = picked[:, base + LANES : base + 2 * LANES]
        qb = picked[:, base + 2 * LANES : base + 3 * LANES]
        sq = jnp.sum(nope * nope + qa * qa * (ROPE / LANES), axis=-1, keepdims=True)
        r = lax.rsqrt(sq * (1.0 / QK) + epsilon)
        q[h] = (nope * r * cut(gq, 0)).astype(bf16)
        turned = (qa * cut(gq, 1) * cos + qb * cut(gq, 2) * sin) * r
        for p in range(pack):
            q[heads + h * pack + p] = jnp.where(
                lane // ROPE == p * heads + h, turned, 0.0
            ).astype(bf16)


def scores_of(heads, q, ref, h, top, count, parts):
    rows = q.shape[1]
    pack = LANES // (ROPE * heads)
    sub = rows // pack
    out = []
    for p in range(parts):
        query = jnp.concatenate(
            [q[h, top : top + count], q[heads + h * pack + p, top : top + count]], axis=1
        )
        key = jnp.concatenate(
            [
                ref[h * rows + p * sub : h * rows + (p + 1) * sub, :],
                ref[heads * rows : heads * rows + sub, :],
            ],
            axis=1,
        )
        out.append(
            lax.dot_general(key, query, (((1,), (1,)), ((), ())), preferred_element_type=f32)
        )
    return out[0] if parts == 1 else jnp.concatenate(out, axis=0)


FACTOR = float(QK ** (-0.5) * np.log2(np.e))


def attend_own(heads, q, ref, state):
    rows = q.shape[1]
    pack = LANES // (ROPE * heads)
    sub = rows // pack
    for h in range(heads):
        for b in range(pack):
            scores = scores_of(heads, q, ref, h, b * sub, sub, b + 1)
            key = lax.broadcasted_iota(jnp.int32, scores.shape, 0)
            query = lax.broadcasted_iota(jnp.int32, scores.shape, 1) + b * sub
            scores = jnp.where(key <= query, scores, -1e30)
            peak = jnp.max(scores, axis=0, keepdims=True)
            weights = jnp.exp2((scores - peak) * FACTOR)
            total = jnp.sum(weights, axis=0, keepdims=True)
            part = dot_rows(ref[h * rows : h * rows + (b + 1) * sub, :], weights.astype(bf16))
            row = lax.broadcasted_iota(jnp.int32, part.shape, 0)
            state[h, :, b * sub : (b + 1) * sub] = jnp.where(
                row == 0, peak, jnp.where(row == 1, total, part)
            )


def attend_other(heads, q, ref, state):
    rows = q.shape[1]
    pack = LANES // (ROPE * heads)
    for h in range(heads):
        scores = scores_of(heads, q, ref, h, 0, rows, pack)
        old = state[h, 0:1, :]
        peak = jnp.maximum(old, jnp.max(scores, axis=0, keepdims=True))
        fade = jnp.exp2((old - peak) * FACTOR)
        weights = jnp.exp2((scores - peak) * FACTOR)
        total = state[h, 1:2, :] * fade + jnp.sum(weights, axis=0, keepdims=True)
        part = dot_rows(ref[h * rows : (h + 1) * rows, :], weights.astype(bf16))
        part = part + state[h] * fade
        row = lax.broadcasted_iota(jnp.int32, part.shape, 0)
        state[h] = jnp.where(row == 0, peak, jnp.where(row == 1, total, part))


def attend_kernel(heads, tokens, groups, q, *refs):
    bundles = refs[:-4]
    keep, send, state, result = refs[-4:]
    me = lax.axis_index("sp")
    core = lax.axis_index("tp") % 2
    attend_own(heads, q, bundles[0], state)
    for k in range(1, len(bundles)):

        @pl.when((me ^ k) < me)
        def _():
            attend_other(heads, q, bundles[k], state)

    outs = [state[h, NOPE:, :] / state[h, 1:2, :] for h in range(heads)]
    result[...] = (outs[0] if heads == 1 else jnp.concatenate(outs, axis=0)).T
    for g in range(groups):
        at = g * 2 * tokens
        keep[g * tokens : (g + 1) * tokens, :] = result[
            pl.ds(pl.multiple_of(at + core * tokens, tokens), tokens), :
        ].astype(bf16)
        send[g * tokens : (g + 1) * tokens, :] = result[
            pl.ds(pl.multiple_of(at + (1 - core) * tokens, tokens), tokens), :
        ].astype(bf16)


def pack_rows(routes, weights, residual, flags, first, second):
    half = second.shape[1]
    rows = [routes[...].astype(f32)]
    for j in range(TOPK):
        rest = weights[j : j + 1, :]
        for _ in range(3):
            piece = rest.astype(bf16).astype(f32)
            rows.append(piece)
            rest = rest - piece
    stacked = jnp.concatenate(rows, axis=0)
    first[:, :half] = residual[:, :half]
    first[:, half:] = dot_rows(stacked.astype(bf16), flags[...]).astype(bf16)
    second[...] = residual[:, half:]


def residual_first_kernel(groups, sp, cap, *refs):
    parts = refs[:groups]
    table, outs, everything = refs[groups], refs[groups + 1 : -1], refs[-1]
    tokens, width = parts[0].shape
    half = width - LANES
    slots = outs[0].shape[0]
    me = lax.axis_index("sp")
    for g in range(groups):
        everything[g * tokens : (g + 1) * tokens, :] = parts[g][...]
    ticket = everything[:, half:].astype(f32)
    lane = lax.broadcasted_iota(jnp.int32, ticket.shape, 1)
    row = lax.broadcasted_iota(jnp.int32, ticket.shape, 0)
    route = [ticket[:, j : j + 1].astype(jnp.int32) for j in range(TOPK)]
    named = me ^ lane
    hit = ((route[0] == named) | (route[1] == named)) & (lane < sp)
    total = groups * tokens
    later = lax.broadcasted_iota(jnp.int32, (total, total), 0)
    earlier = lax.broadcasted_iota(jnp.int32, (total, total), 1)
    lower = (later > earlier) & (later // tokens == earlier // tokens)
    lower = jnp.where(lower, 1.0, 0.0).astype(bf16)
    rank = dot(lower, hit.astype(f32).astype(bf16)).astype(jnp.int32)
    slot = jnp.where(hit, rank + (row // tokens) * cap, -1)
    named = me ^ (lane // 3)
    tail = jnp.zeros(ticket.shape, f32)
    for j in range(TOPK):
        at = TOPK + 3 * j
        piece = jnp.where(
            lane % 3 == 0,
            ticket[:, at : at + 1],
            jnp.where(lane % 3 == 1, ticket[:, at + 1 : at + 2], ticket[:, at + 2 : at + 3]),
        )
        tail = tail + jnp.where((route[j] == named) & (lane < 3 * sp), piece, 0.0)
    everything[:, half:] = tail.astype(bf16)
    place = lax.broadcasted_iota(jnp.int32, (groups * tokens, slots), 1)
    for k, out in enumerate(outs):
        chosen = (slot[:, k : k + 1] == place).astype(f32).astype(bf16)
        table[k] = chosen
        out[...] = dot_rows(chosen, everything[...]).astype(bf16)


def residual_second_kernel(groups, table, *refs):
    parts = refs[:groups]
    outs, everything = refs[groups:-1], refs[-1]
    tokens = parts[0].shape[0]
    for g in range(groups):
        everything[g * tokens : (g + 1) * tokens, :] = parts[g][...]
    for k, out in enumerate(outs):
        out[...] = dot_rows(table[k], everything[...]).astype(bf16)


def choose_kernel(groups, tokens, gain, table, *refs):
    pieces = refs[: 2 * groups]
    outs = refs[2 * groups : -3]
    own, rows_ref, normed_ref = refs[-3:]
    place = lax.axis_index("tp")
    z, core = place // 2, place % 2
    width = 2 * pieces[0].shape[1]
    for g in range(groups):
        mine, other = pieces[2 * g][...].astype(f32), pieces[2 * g + 1][...].astype(f32)
        first = jnp.where(core == 0, mine, other)
        second = jnp.where(core == 0, other, mine)
        at = pl.multiple_of((z ^ g) * width, width)
        rows_ref[:, pl.ds(at, width)] = jnp.concatenate([first, second], axis=1)
    x = rows_ref[...]
    scale = lax.rsqrt(jnp.mean(x * x, axis=-1, keepdims=True) + epsilon)
    normed_ref[...] = (x * scale * gain[...]).astype(bf16)
    blocks = [
        normed_ref[pl.ds(pl.multiple_of((z ^ g) * tokens, tokens), tokens), :]
        for g in range(groups)
    ]
    own[...] = blocks[0]
    near = jnp.concatenate(blocks, axis=0)
    for k, out in enumerate(outs):
        out[...] = dot_rows(table[k], near).astype(bf16)


def expert_kernel(
    part, chunks, own, cap, carried, out_weight, ffn_gain, gate_a, up_a, down_a, gate_b, up_b, down_b, *refs
):
    count = len(part)
    resids, seconds, norms = refs[:count], refs[count : 2 * count], refs[2 * count : 3 * count]
    slots = resids[0].shape[0]
    groups = slots // cap
    results = count * chunks + groups + (1 if own else 0)
    outs, apart = refs[-results:], refs[-results:][count * chunks :][:groups]
    brought = refs[-results - groups : -results] if carried else ()
    total = count * slots
    half = seconds[0].shape[1]
    resid_rows = [jnp.concatenate([r[:, :half], t[...]], axis=1) for r, t in zip(resids, seconds)]
    norm_rows = [n[...] for n in norms]
    if own:
        resid_rows.append(refs[3 * count][...])
        norm_rows.append(refs[3 * count + 1][...])
    join = lambda parts: parts[0] if len(parts) == 1 else jnp.concatenate(parts)
    middle = join(resid_rows).astype(f32) + dot(join(norm_rows), out_weight[...])
    if own:
        outs[-1][...] = middle[total:]
        middle = middle[:total]
    scale = lax.rsqrt(jnp.mean(middle * middle, axis=-1, keepdims=True) + epsilon)
    x = (middle * scale * ffn_gain[...]).astype(bf16)
    hiddens = []
    for gate, up in ((gate_a, up_a), (gate_b, up_b)):
        g = dot(x, gate[0])
        u = dot(x, up[0])
        hiddens.append((g / (1.0 + jnp.exp(-g)) * u).astype(bf16))
    shares = []
    for k, r in zip(part, resids):
        tail = r[:, half:].astype(f32)
        lane = lax.broadcasted_iota(jnp.int32, tail.shape, 1)
        shares.append(jnp.sum(jnp.where(lane // 3 == k, tail, 0.0), axis=-1, keepdims=True))
    weight = join(shares)
    chunk = outs[0].shape[1]
    for j in range(chunks):
        cols = slice(j * chunk, (j + 1) * chunk)
        out = dot(hiddens[0], down_a[0, :, cols]) + dot(hiddens[1], down_b[0, :, cols])
        out = (out * weight).astype(bf16)
        for i in range(count):
            outs[i * chunks + j][...] = out[i * slots : (i + 1) * slots]
    out = dot(hiddens[0], down_a[0, :, chunks * chunk :])
    out = (out + dot(hiddens[1], down_b[0, :, chunks * chunk :])) * weight
    for g in range(groups):
        pieces = [out[i * slots + g * cap : i * slots + (g + 1) * cap] for i in range(count)]
        if carried:
            pieces = [brought[g][...].astype(f32)] + pieces
        apart[g][...] = join(pieces).astype(bf16)


def sum_kernel(groups, cap, *refs):
    parts, outs = refs[:groups], refs[groups:]
    total = parts[0][...].astype(f32)
    for part in parts[1:]:
        total = total + part[...].astype(f32)
    for i, out in enumerate(outs):
        out[...] = total[i * cap : (i + 1) * cap].astype(bf16)


def finish_kernel(sp, tokens, cap, table, middle, *refs):
    rows, out = refs[:sp], refs[sp]
    width = out.shape[1]
    total = middle[:, middle.shape[1] - width :]
    for k in range(sp):
        total = total + dot(table[k, :tokens, :cap], rows[k][...])
    out[...] = total.astype(bf16)


def combine_kernel(sources, tokens, place, chunk, table, *refs):
    rows, outs = refs[:sources], refs[sources:]
    total = None
    for k in range(sources):
        at = 0 if rows[k].shape[1] == chunk else place * chunk
        part = dot(table[k], rows[k][:, at : at + chunk])
        total = part if total is None else total + part
    for g, out in enumerate(outs):
        out[...] = total[g * tokens : (g + 1) * tokens].astype(out.dtype)


VM = pl.BlockSpec(memory_space=pltpu.VMEM)
ANY = pl.BlockSpec(memory_space=pl.ANY)


def call(body, args, outs, scratch=(), after=(), flops=0, trans=0, room=32):
    size = lambda a: int(np.prod(a.shape)) * a.dtype.itemsize
    count = len(args)
    after = list(after)

    def kernel(*refs):
        body(*refs[:count], *refs[count + len(after) :])

    return pl.pallas_call(
        kernel,
        out_shape=outs,
        in_specs=[VM] * count + [ANY] * len(after),
        out_specs=jax.tree.map(lambda _: VM, outs),
        scratch_shapes=list(scratch),
        cost_estimate=pl.CostEstimate(
            flops=int(flops),
            transcendentals=int(trans),
            bytes_accessed=sum(map(size, args)) + sum(map(size, jax.tree.leaves(outs))),
        ),
        compiler_params=pltpu.CompilerParams(vmem_limit_bytes=room * 1024 * 1024),
    )(*args, *after)


def shape(dims, dtype):
    return jax.ShapeDtypeStruct(tuple(dims), dtype)


def program(
    queries, latent, rot_key, latent_gain, key_up, value_up, query_gain, key_gain, out_gain,
    out_weight, residual, ffn_gain, routes, route_weights, expert_gate, expert_up, expert_down,
):
    rows = queries.shape[0]
    heads = key_up.shape[1] // NOPE
    width = residual.shape[1]
    sp, tp = lax.axis_size("sp"), lax.axis_size("tp")
    groups = tp // 2
    tokens = residual.shape[0]
    all_tokens = groups * tokens
    att_width = out_weight.shape[0]
    cap = max(2, 9 * tokens * TOPK // (8 * sp))
    slots = groups * cap

    def swap(v, axis, k, size):
        return lax.ppermute(v, axis, [(i, i ^ k) for i in range(size)])

    def gather_z(v):
        return [v] + [swap_z(v, k) for k in range(1, groups)]

    swap_core = lambda v: swap(v, "tp", 1, tp)
    swap_z = lambda v, k: swap(v, "tp", 2 * k, tp)
    swap_sp = lambda v, k: swap(v, "sp", k, sp)

    flags = np.zeros((4 * TOPK, LANES), np.float32)
    flags[np.arange(4 * TOPK), np.arange(4 * TOPK)] = 1.0

    pack = LANES // (ROPE * heads)
    inner, first = turn_tables(rows, sp)
    selk = jnp.asarray(np.concatenate(rope_select(0, ROPE), axis=1), bf16)
    selq = jnp.asarray(head_select(heads), bf16)
    selg = jnp.asarray(np.abs(head_select(1)), f32)
    bundle, q, first_half, second_half = call(
        functools.partial(prep_kernel, heads),
        [
            latent, rot_key.T, latent_gain[None, :], key_up, value_up, queries.T,
            query_gain[None, :], key_gain[None, :], inner, first, selq, selk, selg,
            routes.T, route_weights.T, residual, jnp.asarray(flags, bf16),
        ],
        (
            shape((heads * rows + rows // pack, LANES), bf16),
            shape((heads * (1 + pack), rows, LANES), bf16),
            shape((tokens, width // 2 + LANES), bf16),
            shape((tokens, width // 2), bf16),
        ),
        flops=2 * rows * latent.shape[1] * 256 + 2 * rows * 192 * 768,
        room=ROOM,
    )
    first_parts = gather_z(first_half)
    second_parts = gather_z(second_half)
    bundles = [bundle] + [swap_sp(bundle, k) for k in range(1, sp)]

    gate_b = swap_core(expert_gate)
    up_b = swap_core(expert_up)
    down_b = swap_core(expert_down)
    table, *first_rows = call(
        functools.partial(residual_first_kernel, groups, sp, cap),
        first_parts,
        (shape((sp, all_tokens, slots), bf16),)
        + tuple([shape((slots, width // 2 + LANES), bf16)] * sp),
        [pltpu.VMEM((all_tokens, width // 2 + LANES), bf16)],
        flops=sp * slots * all_tokens * width,
    )
    first_in = [first_rows[0]] + [swap_sp(first_rows[k], k) for k in range(1, sp)]

    half = heads * VH
    keep, send = call(
        functools.partial(attend_kernel, heads, tokens, groups),
        [q] + bundles,
        (shape((all_tokens, half), bf16), shape((all_tokens, half), bf16)),
        [pltpu.VMEM((heads, LANES, rows), f32), pltpu.VMEM((rows, half), f32)],
        room=ATTEND_ROOM,
        flops=2 * heads * rows * rows * sp * 384,
        trans=heads * rows * rows * sp,
    )
    second_rows = call(
        functools.partial(residual_second_kernel, groups),
        [table] + second_parts,
        tuple([shape((slots, width // 2), bf16)] * sp),
        [pltpu.VMEM((all_tokens, width // 2), bf16)],
        flops=sp * slots * all_tokens * width,
    )
    second_in = [second_rows[0]] + [swap_sp(second_rows[k], k) for k in range(1, sp)]
    other = swap_core(send)
    pieces = []
    for pair in zip(gather_z(keep), gather_z(other)):
        pieces += pair
    *norm_rows, own_rows = call(
        functools.partial(choose_kernel, groups, tokens),
        [out_gain[None, :], table] + pieces,
        tuple([shape((slots, att_width), bf16)] * sp) + (shape((tokens, att_width), bf16),),
        [pltpu.VMEM((all_tokens, att_width), f32), pltpu.VMEM((all_tokens, att_width), bf16)],
        flops=2 * sp * slots * all_tokens * att_width,
    )
    norm_in = [norm_rows[0]] + [swap_sp(norm_rows[k], k) for k in range(1, sp)]

    hidden = 2 * expert_gate.shape[2]
    apart = width // APART
    chunk = (width - apart) // COL_CHUNKS
    parts = expert_parts(sp)
    served, summed = [None] * sp, [None] * sp
    before, carried = [], []
    for n, part in enumerate(parts):
        own, last = n == 0, n == len(parts) - 1
        extra_in = ([residual, own_rows] if own else []) + (carried if last and n else [])
        extra_out = (shape((tokens, width), f32),) if own else ()
        members = ([0] if last and n else []) + part
        cuts = COL_CHUNKS
        outs = call(
            functools.partial(expert_kernel, part, cuts, own, cap, bool(last and n)),
            [
                out_weight, ffn_gain[None, :], expert_gate, expert_up, expert_down,
                gate_b, up_b, down_b,
            ]
            + [first_in[k] for k in part]
            + [second_in[k] for k in part]
            + [norm_in[k] for k in part]
            + extra_in,
            tuple([shape((slots, chunk * COL_CHUNKS // cuts), bf16)] * (len(part) * cuts))
            + tuple([shape((len(members) * cap, apart), bf16)] * groups)
            + extra_out,
            after=before,
            flops=2 * len(part) * slots * width * (att_width + 3 * hidden),
        )
        before = [outs[0]]
        for i, k in enumerate(part):
            served[k] = [swap_sp(v, k) if k else v for v in outs[i * cuts : (i + 1) * cuts]]
        split = outs[len(part) * cuts :][:groups]
        if own:
            middle = outs[-1]
            carried = list(split)
        if not own or last:
            sums = call(
                functools.partial(sum_kernel, groups, cap),
                [split[0]] + [swap_z(split[k], k) for k in range(1, groups)],
                tuple([shape((cap, apart), bf16)] * len(members)),
            )
            for k, v in zip(members, sums):
                summed[k] = swap_sp(v, k) if k else v
    finished = []
    for j in range(COL_CHUNKS):
        back = [v[min(j, len(v) - 1)] for v in served]
        own, *rest = call(
            functools.partial(combine_kernel, sp, tokens, j, chunk),
            [table] + back,
            (shape((tokens, chunk), f32),) + tuple([shape((tokens, chunk), bf16)] * (groups - 1)),
            flops=2 * all_tokens * sp * slots * chunk,
        )
        total = middle[:, j * chunk : (j + 1) * chunk] + own
        for k in range(1, groups):
            total = total + swap_z(rest[k - 1], k).astype(f32)
        finished.append(total.astype(bf16))
    finished.append(
        call(
            functools.partial(finish_kernel, sp, tokens, cap),
            [table, middle] + summed,
            shape((tokens, apart), bf16),
        )
    )
    return jnp.concatenate(finished, axis=1)


def expert_parts(sp):
    parts, at = [[0], [k for k in (1, 2) if k < sp]], 3
    while at < sp:
        parts.append(list(range(at, min(at + 4, sp))))
        at += 4
    return [p for p in parts if p]


def solution(mesh):
    return jax.shard_map(
        program,
        mesh=mesh,
        in_specs=(
            P("sp", "tp"),
            P("sp", None),
            P("sp", None),
            P(),
            P(None, "tp"),
            P(None, "tp"),
            P(),
            P(),
            P(),
            P(),
            P(("sp", "tp"), None),
            P(),
            P(("sp", "tp"), None),
            P(("sp", "tp"), None),
            P("sp", None, "tp"),
            P("sp", None, "tp"),
            P("sp", "tp", None),
        ),
        out_specs=P(("sp", "tp"), None),
        check_vma=False,
    )
```

```python
import functools

import jax
import jax.numpy as jnp
import numpy as np
from jax import lax
from jax.experimental import pallas as pl
from jax.experimental.pallas import tpu as pltpu
from jax.sharding import PartitionSpec as P


NOPE = 64
ROPE = 32
VH = 64
TOPK = 2
QK = 96
LANES = 128
COL_CHUNKS = 2
APART = 4
ROOM = 60
ATTEND_ROOM = 44


epsilon = 1e-06
rope_base = 10000.0
f32 = jnp.float32
bf16 = jnp.bfloat16


def dot(a, b):
    return jnp.dot(a, b, preferred_element_type=f32)


def rope_select(offset, rows):
    direct = np.zeros((rows, LANES), np.float32)
    turned = np.zeros((rows, LANES), np.float32)
    half = ROPE // 2
    for lane in range(LANES):
        d = lane % ROPE
        direct[offset + d, lane] = 1.0
        turned[offset + (d + half) % ROPE, lane] = -1.0 if d < half else 1.0
    return direct, turned


def head_select(heads):
    parts = []
    for h in range(heads):
        nope = np.zeros((heads * QK, LANES), np.float32)
        for i in range(NOPE):
            nope[h * QK + i, i] = 1.0
        parts += [nope, *rope_select(h * QK + NOPE, heads * QK)]
    return np.concatenate(parts, axis=1)


def turn_tables(rows, blocks):
    inverse = rope_base ** (-np.arange(0, ROPE, 2, dtype=np.float64) / ROPE)
    inverse = np.tile(inverse, 2 * LANES // ROPE)[None, :]
    inner = np.arange(rows, dtype=np.float64)[:, None] * inverse
    first = np.arange(blocks, dtype=np.float64)[:, None] * rows * inverse
    return [
        np.concatenate([np.cos(a), np.sin(a)], axis=1).astype(np.float32) for a in (inner, first)
    ]


def dot_rows(a, b):
    return lax.dot_general(a, b, (((0,), (0,)), ((), ())), preferred_element_type=f32)


def prep_kernel(
    heads, lat, rot, lat_gain, key_up, value_up, queries, q_gain, k_gain, inner, first,
    selq, selk, selg, routes, route_weights, residual, flags, bundle, q, head, rest,
):
    pack_rows(routes, route_weights, residual, flags, head, rest)
    rows = lat.shape[0]
    pack = LANES // (ROPE * heads)
    sub = rows // pack
    me = lax.axis_index("sp")
    x = lat[...].astype(f32)
    scale = lax.rsqrt(jnp.mean(x * x, axis=-1, keepdims=True) + epsilon)
    normed = (x * scale * lat_gain[...]).astype(bf16)
    base = first[pl.ds(me, 1), :]
    base_cos, base_sin = base[:, :LANES], base[:, LANES:]
    in_cos, in_sin = inner[:, :LANES], inner[:, LANES:]
    cos = in_cos * base_cos - in_sin * base_sin
    sin = in_sin * base_cos + in_cos * base_sin
    spread_gain = lambda g: jnp.dot(
        g[...], selg[...], precision=lax.Precision.HIGHEST, preferred_element_type=f32
    )
    gq, gk = spread_gain(q_gain), spread_gain(k_gain)
    cut = lambda g, i: g[:, i * LANES : (i + 1) * LANES]
    lane = lax.broadcasted_iota(jnp.int32, (rows, LANES), 1)
    is_key = lane < NOPE
    turns = dot_rows(rot[...], selk[...])
    rot_a, rot_b = turns[:, :LANES], turns[:, LANES:]
    rot_sq = jnp.sum(rot_a * rot_a, axis=-1, keepdims=True) * (ROPE / LANES)
    spun = rot_a * cut(gk, 1) * cos + rot_b * cut(gk, 2) * sin
    key_scales = None
    for h in range(heads):
        weight = jnp.concatenate(
            [key_up[:, h * NOPE : (h + 1) * NOPE], value_up[:, h * VH : (h + 1) * VH]], axis=1
        )
        kv = dot(normed, weight).astype(bf16).astype(f32)
        sq = jnp.sum(jnp.where(is_key, kv * kv, 0.0), axis=-1, keepdims=True) + rot_sq
        r = lax.rsqrt(sq * (1.0 / QK) + epsilon)
        bundle[h * rows : (h + 1) * rows, :] = jnp.where(
            is_key, kv * r * cut(gk, 0), kv
        ).astype(bf16)
        spread = jnp.broadcast_to(r, (rows, LANES))
        key_scales = (
            spread
            if key_scales is None
            else jnp.where((lane // ROPE) % heads == h, spread, key_scales)
        )
    spun = spun * key_scales
    tile = spun[:sub]
    for p in range(1, pack):
        tile = jnp.where(
            lane[:sub] // (ROPE * heads) == p, spun[p * sub : (p + 1) * sub], tile
        )
    bundle[heads * rows :, :] = tile.astype(bf16)
    picked = dot_rows(queries[...], selq[...])
    for h in range(heads):
        base = h * 3 * LANES
        nope = picked[:, base : base + LANES]
        qa = picked[:, base + LANES : base + 2 * LANES]
        qb = picked[:, base + 2 * LANES : base + 3 * LANES]
        sq = jnp.sum(nope * nope + qa * qa * (ROPE / LANES), axis=-1, keepdims=True)
        r = lax.rsqrt(sq * (1.0 / QK) + epsilon)
        q[h] = (nope * r * cut(gq, 0)).astype(bf16)
        turned = (qa * cut(gq, 1) * cos + qb * cut(gq, 2) * sin) * r
        for p in range(pack):
            q[heads + h * pack + p] = jnp.where(
                lane // ROPE == p * heads + h, turned, 0.0
            ).astype(bf16)


def scores_of(heads, q, ref, h, top, count, parts):
    rows = q.shape[1]
    pack = LANES // (ROPE * heads)
    sub = rows // pack
    out = []
    for p in range(parts):
        query = jnp.concatenate(
            [q[h, top : top + count], q[heads + h * pack + p, top : top + count]], axis=1
        )
        key = jnp.concatenate(
            [
                ref[h * rows + p * sub : h * rows + (p + 1) * sub, :],
                ref[heads * rows : heads * rows + sub, :],
            ],
            axis=1,
        )
        out.append(
            lax.dot_general(key, query, (((1,), (1,)), ((), ())), preferred_element_type=f32)
        )
    return out[0] if parts == 1 else jnp.concatenate(out, axis=0)


FACTOR = float(QK ** (-0.5) * np.log2(np.e))


def attend_own(heads, q, ref, state):
    rows = q.shape[1]
    pack = LANES // (ROPE * heads)
    sub = rows // pack
    for h in range(heads):
        for b in range(pack):
            scores = scores_of(heads, q, ref, h, b * sub, sub, b + 1)
            key = lax.broadcasted_iota(jnp.int32, scores.shape, 0)
            query = lax.broadcasted_iota(jnp.int32, scores.shape, 1) + b * sub
            scores = jnp.where(key <= query, scores, -1e30)
            peak = jnp.max(scores, axis=0, keepdims=True)
            weights = jnp.exp2((scores - peak) * FACTOR)
            total = jnp.sum(weights, axis=0, keepdims=True)
            part = dot_rows(ref[h * rows : h * rows + (b + 1) * sub, :], weights.astype(bf16))
            row = lax.broadcasted_iota(jnp.int32, part.shape, 0)
            state[h, :, b * sub : (b + 1) * sub] = jnp.where(
                row == 0, peak, jnp.where(row == 1, total, part)
            )


def attend_other(heads, q, ref, state):
    rows = q.shape[1]
    pack = LANES // (ROPE * heads)
    for h in range(heads):
        scores = scores_of(heads, q, ref, h, 0, rows, pack)
        old = state[h, 0:1, :]
        peak = jnp.maximum(old, jnp.max(scores, axis=0, keepdims=True))
        fade = jnp.exp2((old - peak) * FACTOR)
        weights = jnp.exp2((scores - peak) * FACTOR)
        total = state[h, 1:2, :] * fade + jnp.sum(weights, axis=0, keepdims=True)
        part = dot_rows(ref[h * rows : (h + 1) * rows, :], weights.astype(bf16))
        part = part + state[h] * fade
        row = lax.broadcasted_iota(jnp.int32, part.shape, 0)
        state[h] = jnp.where(row == 0, peak, jnp.where(row == 1, total, part))


def attend_kernel(heads, tokens, groups, q, *refs):
    bundles = refs[:-4]
    keep, send, state, result = refs[-4:]
    me = lax.axis_index("sp")
    core = lax.axis_index("tp") % 2
    attend_own(heads, q, bundles[0], state)
    for k in range(1, len(bundles)):

        @pl.when((me ^ k) < me)
        def _():
            attend_other(heads, q, bundles[k], state)

    outs = [state[h, NOPE:, :] / state[h, 1:2, :] for h in range(heads)]
    result[...] = (outs[0] if heads == 1 else jnp.concatenate(outs, axis=0)).T
    for g in range(groups):
        at = g * 2 * tokens
        keep[g * tokens : (g + 1) * tokens, :] = result[
            pl.ds(pl.multiple_of(at + core * tokens, tokens), tokens), :
        ].astype(bf16)
        send[g * tokens : (g + 1) * tokens, :] = result[
            pl.ds(pl.multiple_of(at + (1 - core) * tokens, tokens), tokens), :
        ].astype(bf16)


def pack_rows(routes, weights, residual, flags, first, second):
    half = second.shape[1]
    rows = [routes[...].astype(f32)]
    for j in range(TOPK):
        rest = weights[j : j + 1, :]
        for _ in range(3):
            piece = rest.astype(bf16).astype(f32)
            rows.append(piece)
            rest = rest - piece
    stacked = jnp.concatenate(rows, axis=0)
    first[:, :half] = residual[:, :half]
    first[:, half:] = dot_rows(stacked.astype(bf16), flags[...]).astype(bf16)
    second[...] = residual[:, half:]


def residual_first_kernel(groups, sp, cap, *refs):
    parts = refs[:groups]
    table, outs, everything = refs[groups], refs[groups + 1 : -1], refs[-1]
    tokens, width = parts[0].shape
    half = width - LANES
    slots = outs[0].shape[0]
    me = lax.axis_index("sp")
    for g in range(groups):
        everything[g * tokens : (g + 1) * tokens, :] = parts[g][...]
    ticket = everything[:, half:].astype(f32)
    lane = lax.broadcasted_iota(jnp.int32, ticket.shape, 1)
    row = lax.broadcasted_iota(jnp.int32, ticket.shape, 0)
    route = [ticket[:, j : j + 1].astype(jnp.int32) for j in range(TOPK)]
    named = me ^ lane
    hit = ((route[0] == named) | (route[1] == named)) & (lane < sp)
    total = groups * tokens
    later = lax.broadcasted_iota(jnp.int32, (total, total), 0)
    earlier = lax.broadcasted_iota(jnp.int32, (total, total), 1)
    lower = (later > earlier) & (later // tokens == earlier // tokens)
    lower = jnp.where(lower, 1.0, 0.0).astype(bf16)
    rank = dot(lower, hit.astype(f32).astype(bf16)).astype(jnp.int32)
    slot = jnp.where(hit, rank + (row // tokens) * cap, -1)
    named = me ^ (lane // 3)
    tail = jnp.zeros(ticket.shape, f32)
    for j in range(TOPK):
        at = TOPK + 3 * j
        piece = jnp.where(
            lane % 3 == 0,
            ticket[:, at : at + 1],
            jnp.where(lane % 3 == 1, ticket[:, at + 1 : at + 2], ticket[:, at + 2 : at + 3]),
        )
        tail = tail + jnp.where((route[j] == named) & (lane < 3 * sp), piece, 0.0)
    everything[:, half:] = tail.astype(bf16)
    place = lax.broadcasted_iota(jnp.int32, (groups * tokens, slots), 1)
    for k, out in enumerate(outs):
        chosen = (slot[:, k : k + 1] == place).astype(f32).astype(bf16)
        table[k] = chosen
        out[...] = dot_rows(chosen, everything[...]).astype(bf16)


def residual_second_kernel(groups, table, *refs):
    parts = refs[:groups]
    outs, everything = refs[groups:-1], refs[-1]
    tokens = parts[0].shape[0]
    for g in range(groups):
        everything[g * tokens : (g + 1) * tokens, :] = parts[g][...]
    for k, out in enumerate(outs):
        out[...] = dot_rows(table[k], everything[...]).astype(bf16)


def choose_kernel(groups, tokens, gain, table, *refs):
    pieces = refs[: 2 * groups]
    outs = refs[2 * groups : -3]
    own, rows_ref, normed_ref = refs[-3:]
    place = lax.axis_index("tp")
    z, core = place // 2, place % 2
    width = 2 * pieces[0].shape[1]
    for g in range(groups):
        mine, other = pieces[2 * g][...].astype(f32), pieces[2 * g + 1][...].astype(f32)
        first = jnp.where(core == 0, mine, other)
        second = jnp.where(core == 0, other, mine)
        at = pl.multiple_of((z ^ g) * width, width)
        rows_ref[:, pl.ds(at, width)] = jnp.concatenate([first, second], axis=1)
    x = rows_ref[...]
    scale = lax.rsqrt(jnp.mean(x * x, axis=-1, keepdims=True) + epsilon)
    normed_ref[...] = (x * scale * gain[...]).astype(bf16)
    blocks = [
        normed_ref[pl.ds(pl.multiple_of((z ^ g) * tokens, tokens), tokens), :]
        for g in range(groups)
    ]
    own[...] = blocks[0]
    near = jnp.concatenate(blocks, axis=0)
    for k, out in enumerate(outs):
        out[...] = dot_rows(table[k], near).astype(bf16)


def expert_kernel(
    part, chunks, own, cap, carried, out_weight, ffn_gain, gate_a, up_a, down_a, gate_b, up_b, down_b, *refs
):
    count = len(part)
    resids, seconds, norms = refs[:count], refs[count : 2 * count], refs[2 * count : 3 * count]
    slots = resids[0].shape[0]
    groups = slots // cap
    results = count * chunks + groups + (1 if own else 0)
    outs, apart = refs[-results:], refs[-results:][count * chunks :][:groups]
    brought = refs[-results - groups : -results] if carried else ()
    total = count * slots
    half = seconds[0].shape[1]
    resid_rows = [jnp.concatenate([r[:, :half], t[...]], axis=1) for r, t in zip(resids, seconds)]
    norm_rows = [n[...] for n in norms]
    if own:
        resid_rows.append(refs[3 * count][...])
        norm_rows.append(refs[3 * count + 1][...])
    join = lambda parts: parts[0] if len(parts) == 1 else jnp.concatenate(parts)
    middle = join(resid_rows).astype(f32) + dot(join(norm_rows), out_weight[...])
    if own:
        outs[-1][...] = middle[total:]
        middle = middle[:total]
    scale = lax.rsqrt(jnp.mean(middle * middle, axis=-1, keepdims=True) + epsilon)
    x = (middle * scale * ffn_gain[...]).astype(bf16)
    hiddens = []
    for gate, up in ((gate_a, up_a), (gate_b, up_b)):
        g = dot(x, gate[0])
        u = dot(x, up[0])
        hiddens.append((g / (1.0 + jnp.exp(-g)) * u).astype(bf16))
    shares = []
    for k, r in zip(part, resids):
        tail = r[:, half:].astype(f32)
        lane = lax.broadcasted_iota(jnp.int32, tail.shape, 1)
        shares.append(jnp.sum(jnp.where(lane // 3 == k, tail, 0.0), axis=-1, keepdims=True))
    weight = join(shares)
    chunk = outs[0].shape[1]
    for j in range(chunks):
        cols = slice(j * chunk, (j + 1) * chunk)
        out = dot(hiddens[0], down_a[0, :, cols]) + dot(hiddens[1], down_b[0, :, cols])
        out = (out * weight).astype(bf16)
        for i in range(count):
            outs[i * chunks + j][...] = out[i * slots : (i + 1) * slots]
    out = dot(hiddens[0], down_a[0, :, chunks * chunk :])
    out = (out + dot(hiddens[1], down_b[0, :, chunks * chunk :])) * weight
    for g in range(groups):
        pieces = [out[i * slots + g * cap : i * slots + (g + 1) * cap] for i in range(count)]
        if carried:
            pieces = [brought[g][...].astype(f32)] + pieces
        apart[g][...] = join(pieces).astype(bf16)


def sum_kernel(groups, cap, *refs):
    parts, outs = refs[:groups], refs[groups:]
    total = parts[0][...].astype(f32)
    for part in parts[1:]:
        total = total + part[...].astype(f32)
    for i, out in enumerate(outs):
        out[...] = total[i * cap : (i + 1) * cap].astype(bf16)


def finish_kernel(sp, tokens, cap, chunks, table, middle, *refs):
    rows, owns, far, out = refs[:sp], refs[sp : sp + chunks], refs[sp + chunks : -1], refs[-1]
    each = len(far) // chunks
    chunk = owns[0].shape[1]
    for j in range(chunks):
        cols = slice(j * chunk, (j + 1) * chunk)
        total = middle[:, cols] + owns[j][...]
        for part in far[j * each : (j + 1) * each]:
            total = total + part[...].astype(f32)
        out[:, cols] = total.astype(bf16)
    total = middle[:, chunks * chunk :]
    for k in range(sp):
        total = total + dot(table[k, :tokens, :cap], rows[k][...])
    out[:, chunks * chunk :] = total.astype(bf16)


def combine_kernel(sources, tokens, place, chunk, table, *refs):
    rows, outs = refs[:sources], refs[sources:]
    total = None
    for k in range(sources):
        at = 0 if rows[k].shape[1] == chunk else place * chunk
        part = dot(table[k], rows[k][:, at : at + chunk])
        total = part if total is None else total + part
    for g, out in enumerate(outs):
        out[...] = total[g * tokens : (g + 1) * tokens].astype(out.dtype)


VM = pl.BlockSpec(memory_space=pltpu.VMEM)
ANY = pl.BlockSpec(memory_space=pl.ANY)


def call(body, args, outs, scratch=(), after=(), flops=0, trans=0, room=32):
    size = lambda a: int(np.prod(a.shape)) * a.dtype.itemsize
    count = len(args)
    after = list(after)

    def kernel(*refs):
        body(*refs[:count], *refs[count + len(after) :])

    return pl.pallas_call(
        kernel,
        out_shape=outs,
        in_specs=[VM] * count + [ANY] * len(after),
        out_specs=jax.tree.map(lambda _: VM, outs),
        scratch_shapes=list(scratch),
        cost_estimate=pl.CostEstimate(
            flops=int(flops),
            transcendentals=int(trans),
            bytes_accessed=sum(map(size, args)) + sum(map(size, jax.tree.leaves(outs))),
        ),
        compiler_params=pltpu.CompilerParams(vmem_limit_bytes=room * 1024 * 1024),
    )(*args, *after)


def shape(dims, dtype):
    return jax.ShapeDtypeStruct(tuple(dims), dtype)


def program(
    queries, latent, rot_key, latent_gain, key_up, value_up, query_gain, key_gain, out_gain,
    out_weight, residual, ffn_gain, routes, route_weights, expert_gate, expert_up, expert_down,
):
    rows = queries.shape[0]
    heads = key_up.shape[1] // NOPE
    width = residual.shape[1]
    sp, tp = lax.axis_size("sp"), lax.axis_size("tp")
    groups = tp // 2
    tokens = residual.shape[0]
    all_tokens = groups * tokens
    att_width = out_weight.shape[0]
    cap = max(2, 9 * tokens * TOPK // (8 * sp))
    slots = groups * cap

    def swap(v, axis, k, size):
        return lax.ppermute(v, axis, [(i, i ^ k) for i in range(size)])

    def gather_z(v):
        return [v] + [swap_z(v, k) for k in range(1, groups)]

    swap_core = lambda v: swap(v, "tp", 1, tp)
    swap_z = lambda v, k: swap(v, "tp", 2 * k, tp)
    swap_sp = lambda v, k: swap(v, "sp", k, sp)

    flags = np.zeros((4 * TOPK, LANES), np.float32)
    flags[np.arange(4 * TOPK), np.arange(4 * TOPK)] = 1.0

    pack = LANES // (ROPE * heads)
    inner, first = turn_tables(rows, sp)
    selk = jnp.asarray(np.concatenate(rope_select(0, ROPE), axis=1), bf16)
    selq = jnp.asarray(head_select(heads), bf16)
    selg = jnp.asarray(np.abs(head_select(1)), f32)
    bundle, q, first_half, second_half = call(
        functools.partial(prep_kernel, heads),
        [
            latent, rot_key.T, latent_gain[None, :], key_up, value_up, queries.T,
            query_gain[None, :], key_gain[None, :], inner, first, selq, selk, selg,
            routes.T, route_weights.T, residual, jnp.asarray(flags, bf16),
        ],
        (
            shape((heads * rows + rows // pack, LANES), bf16),
            shape((heads * (1 + pack), rows, LANES), bf16),
            shape((tokens, width // 2 + LANES), bf16),
            shape((tokens, width // 2), bf16),
        ),
        flops=2 * rows * latent.shape[1] * 256 + 2 * rows * 192 * 768,
        room=ROOM,
    )
    first_parts = gather_z(first_half)
    second_parts = gather_z(second_half)
    bundles = [bundle] + [swap_sp(bundle, k) for k in range(1, sp)]

    gate_b = swap_core(expert_gate)
    up_b = swap_core(expert_up)
    down_b = swap_core(expert_down)
    table, *first_rows = call(
        functools.partial(residual_first_kernel, groups, sp, cap),
        first_parts,
        (shape((sp, all_tokens, slots), bf16),)
        + tuple([shape((slots, width // 2 + LANES), bf16)] * sp),
        [pltpu.VMEM((all_tokens, width // 2 + LANES), bf16)],
        flops=sp * slots * all_tokens * width,
    )
    first_in = [first_rows[0]] + [swap_sp(first_rows[k], k) for k in range(1, sp)]

    half = heads * VH
    keep, send = call(
        functools.partial(attend_kernel, heads, tokens, groups),
        [q] + bundles,
        (shape((all_tokens, half), bf16), shape((all_tokens, half), bf16)),
        [pltpu.VMEM((heads, LANES, rows), f32), pltpu.VMEM((rows, half), f32)],
        room=ATTEND_ROOM,
        flops=2 * heads * rows * rows * sp * 384,
        trans=heads * rows * rows * sp,
    )
    second_rows = call(
        functools.partial(residual_second_kernel, groups),
        [table] + second_parts,
        tuple([shape((slots, width // 2), bf16)] * sp),
        [pltpu.VMEM((all_tokens, width // 2), bf16)],
        flops=sp * slots * all_tokens * width,
    )
    second_in = [second_rows[0]] + [swap_sp(second_rows[k], k) for k in range(1, sp)]
    other = swap_core(send)
    pieces = []
    for pair in zip(gather_z(keep), gather_z(other)):
        pieces += pair
    *norm_rows, own_rows = call(
        functools.partial(choose_kernel, groups, tokens),
        [out_gain[None, :], table] + pieces,
        tuple([shape((slots, att_width), bf16)] * sp) + (shape((tokens, att_width), bf16),),
        [pltpu.VMEM((all_tokens, att_width), f32), pltpu.VMEM((all_tokens, att_width), bf16)],
        flops=2 * sp * slots * all_tokens * att_width,
    )
    norm_in = [norm_rows[0]] + [swap_sp(norm_rows[k], k) for k in range(1, sp)]

    hidden = 2 * expert_gate.shape[2]
    apart = width // APART
    chunk = (width - apart) // COL_CHUNKS
    parts = expert_parts(sp)
    served, summed = [None] * sp, [None] * sp
    before, carried = [], []
    for n, part in enumerate(parts):
        own, last = n == 0, n == len(parts) - 1
        extra_in = ([residual, own_rows] if own else []) + (carried if last and n else [])
        extra_out = (shape((tokens, width), f32),) if own else ()
        members = ([0] if last and n else []) + part
        cuts = COL_CHUNKS
        outs = call(
            functools.partial(expert_kernel, part, cuts, own, cap, bool(last and n)),
            [
                out_weight, ffn_gain[None, :], expert_gate, expert_up, expert_down,
                gate_b, up_b, down_b,
            ]
            + [first_in[k] for k in part]
            + [second_in[k] for k in part]
            + [norm_in[k] for k in part]
            + extra_in,
            tuple([shape((slots, chunk * COL_CHUNKS // cuts), bf16)] * (len(part) * cuts))
            + tuple([shape((len(members) * cap, apart), bf16)] * groups)
            + extra_out,
            after=before,
            flops=2 * len(part) * slots * width * (att_width + 3 * hidden),
        )
        before = [outs[0]]
        for i, k in enumerate(part):
            served[k] = [swap_sp(v, k) if k else v for v in outs[i * cuts : (i + 1) * cuts]]
        split = outs[len(part) * cuts :][:groups]
        if own:
            middle = outs[-1]
            carried = list(split)
        if not own or last:
            sums = call(
                functools.partial(sum_kernel, groups, cap),
                [split[0]] + [swap_z(split[k], k) for k in range(1, groups)],
                tuple([shape((cap, apart), bf16)] * len(members)),
            )
            for k, v in zip(members, sums):
                summed[k] = swap_sp(v, k) if k else v
    owns, far = [], []
    for j in range(COL_CHUNKS):
        back = [v[min(j, len(v) - 1)] for v in served]
        own, *rest = call(
            functools.partial(combine_kernel, sp, tokens, j, chunk),
            [table] + back,
            (shape((tokens, chunk), f32),) + tuple([shape((tokens, chunk), bf16)] * (groups - 1)),
            flops=2 * all_tokens * sp * slots * chunk,
        )
        owns.append(own)
        far += [swap_z(rest[k - 1], k) for k in range(1, groups)]
    return call(
        functools.partial(finish_kernel, sp, tokens, cap, COL_CHUNKS),
        [table, middle] + summed + owns + far,
        shape((tokens, width), bf16),
    )


def expert_parts(sp):
    parts, at = [[0], [k for k in (1, 2) if k < sp]], 3
    while at < sp:
        parts.append(list(range(at, min(at + 4, sp))))
        at += 4
    return [p for p in parts if p]


def solution(mesh):
    return jax.shard_map(
        program,
        mesh=mesh,
        in_specs=(
            P("sp", "tp"),
            P("sp", None),
            P("sp", None),
            P(),
            P(None, "tp"),
            P(None, "tp"),
            P(),
            P(),
            P(),
            P(),
            P(("sp", "tp"), None),
            P(),
            P(("sp", "tp"), None),
            P(("sp", "tp"), None),
            P("sp", None, "tp"),
            P("sp", None, "tp"),
            P("sp", "tp", None),
        ),
        out_specs=P(("sp", "tp"), None),
        check_vma=False,
    )
```
